32 devices in a mesh: sp: 4 (over z), fs: 4 (over y, x), tp: 2 (over core).
Axes of the slice: x: 2, y: 2, z: 4, core: 2. Of those that a mesh axis runs over, the one named last changes fastest.
Arguments:
- tokens: bfloat16 [4, 1024, 2048], P('fs', 'sp'), may hold values from -6 to 6
- norm_gain: float32 [2048], replicated, may hold values from 0.1 to 1.9
- query_weight: bfloat16 [2048, 1024], P(('sp', 'fs'), 'tp'), may hold values from -0.125 to 0.125
- key_weight: bfloat16 [2048, 1024], P(('sp', 'fs'), 'tp'), may hold values from -0.125 to 0.125
- value_weight: bfloat16 [2048, 1024], P(('sp', 'fs'), 'tp'), may hold values from -0.125 to 0.125
- outgate_weight: bfloat16 [2048, 1024], P(('sp', 'fs'), 'tp'), may hold values from -0.125 to 0.125
- gate_weight: bfloat16 [4, 8, 2048], P(None, 'tp'), may hold values from -0.125 to 0.125
- gate_bias: float32 [4, 8], P(None, 'tp'), may hold values from -1 to 100
- decay_extra: float32 [4, 2, 8, 1024], P('fs', None, 'tp', 'sp'), may hold values from -0.75 to 0
- init_memory: float32 [4, 2, 8, 128, 128], P('fs', None, 'tp'), may hold values from -48 to 48
- init_normalizer: float32 [4, 2, 8, 128], P('fs', None, 'tp'), may hold values from -48 to 48
- head_gain: float32 [8, 128], P('tp'), may hold values from 0.1 to 1.9
- pool_weight: bfloat16 [2048, 2048], P(('sp', 'fs'), 'tp'), may hold values from -0.125 to 0.125
- mem_out_weight: bfloat16 [2048, 1024], P(('sp', 'fs'), 'tp'), may hold values from -0.1875 to 0.1875
- pool_out_weight: bfloat16 [2048, 2048], P(('sp', 'fs'), 'tp'), may hold values from -0.125 to 0.125
Outputs:
- mixed: bfloat16 [4, 1024, 2048], P('fs', ('sp', 'tp'))
The draws below stay inside these ranges and needn't reach their ends.
All inputs are finite; a program needn't handle non-finite values.
Results may differ from the reference program's by a relative error of at most 0.014.
Values may be sent and summed in bfloat16 or wider, within the bound.
A program may use at most 64 MiB of HBM per device.

```python
import math
from functools import partial
import jax
import jax.numpy as jnp
from jax import lax

D = 2048
MEMORY_HEADS = 8
HEAD_DIM = 128
HALO = 8
T_DEV = 256
MEM_W = 1024
TOKEN_LENGTH = 1024
SEQUENCE_COUNT = 4
N_TP = 2


def draw_gate_bias(key, part):
    rank_key, slow_key, fast_key, input_key, pick_key, strong_key = jax.random.split(key, 6)
    ranking = jax.random.permutation(rank_key, MEMORY_HEADS)
    picking = jax.random.permutation(pick_key, MEMORY_HEADS)
    slow_heads = ranking < MEMORY_HEADS // 2
    strong_heads = picking < 0
    slow_bias = math.log(3.3 * TOKEN_LENGTH) + jax.random.uniform(slow_key, (2, MEMORY_HEADS), jnp.float32, 0.0, 0.5)
    fast_bias = jax.random.uniform(fast_key, (2, MEMORY_HEADS), jnp.float32, math.log(50.0), math.log(165.0))
    forget_bias = jnp.where(slow_heads[None, :], slow_bias, fast_bias)
    gentle = jax.random.uniform(input_key, (2, MEMORY_HEADS), jnp.float32, -1.0, 1.0)
    strong_bias = jax.random.uniform(strong_key, (2, MEMORY_HEADS), jnp.float32, 80.0, 100.0)
    input_bias = jnp.where(strong_heads[None, :], strong_bias, gentle)
    return jnp.stack([input_bias[0], forget_bias[0], input_bias[1], forget_bias[1]]).astype(jnp.float32)


def draw_decay_extra(key, part):
    speed_key, spike_key, penalty_key = jax.random.split(key, 3)
    block_count = TOKEN_LENGTH // T_DEV
    rates = jnp.exp(jax.random.uniform(speed_key, (SEQUENCE_COUNT, 2, MEMORY_HEADS, block_count), jnp.float32, math.log(0.25), math.log(2.0)))
    stable_values = -0.5 / TOKEN_LENGTH * jnp.repeat(rates, T_DEV, axis=-1)
    spike_values = jax.random.bernoulli(spike_key, 2.0 / TOKEN_LENGTH, (SEQUENCE_COUNT, 2, MEMORY_HEADS, TOKEN_LENGTH))
    penalty_values = jax.random.uniform(penalty_key, (SEQUENCE_COUNT, 2, MEMORY_HEADS, TOKEN_LENGTH), jnp.float32, math.log(0.5), math.log(0.8))
    return (stable_values + jnp.where(spike_values, penalty_values, 0.0)).astype(jnp.float32)


def shard_levels(rng, shape, shards, least, high):
    def one(position, shards_of):
        steps = jax.random.uniform(jax.random.fold_in(jax.random.fold_in(rng, 6), position), (shards_of,), jnp.float32, least / len(shards), high / len(shards))
        return jnp.repeat(jnp.exp(steps), shape[position] // shards_of).reshape((-1,) + (1,) * (len(shape) - position - 1))

    level = one(*shards[0])
    for cut in shards[1:]:
        level = level * one(*cut)
    return level


def gaussian(key, extent, spread, bound, cuts=(), held_as=jnp.bfloat16):
    gain = shard_levels(key, extent, cuts, -0.22, 0.18) if cuts else 1.0
    drawn = jax.random.normal(key, extent, jnp.float32) * spread * gain
    return jnp.minimum(jnp.maximum(drawn, -bound), bound).astype(held_as)


def setup_inputs(seed: int = 0) -> dict:
    streams_of = jax.random.split(jax.random.key(seed), 16)
    tokens = gaussian(streams_of[0], (SEQUENCE_COUNT, TOKEN_LENGTH, D), 1.0, 6.0, ((0, 4), (1, 4)))
    norm_gain = jnp.clip(1.0 + 0.18 * jax.random.normal(streams_of[1], (D,), jnp.float32), 0.1, 1.9)
    query_weight = gaussian(streams_of[2], (D, MEM_W), D ** -0.5, 0.125, ((0, 16), (1, 2)))
    key_weight = gaussian(streams_of[3], (D, MEM_W), D ** -0.5, 0.125, ((0, 16), (1, 2)))
    value_weight = gaussian(streams_of[4], (D, MEM_W), D ** -0.5, 0.125, ((0, 16), (1, 2)))
    outgate_weight = gaussian(streams_of[5], (D, MEM_W), D ** -0.5, 0.125, ((0, 16), (1, 2)))
    gate_weight = gaussian(streams_of[6], (4, MEMORY_HEADS, D), D ** -0.5, 0.125, ((1, 2),))
    gate_bias = draw_gate_bias(jax.random.fold_in(streams_of[15], 71), 0)
    decay_extra = draw_decay_extra(jax.random.fold_in(streams_of[15], 71), 0)
    init_memory = gaussian(streams_of[9], (SEQUENCE_COUNT, 2, MEMORY_HEADS, HEAD_DIM, HEAD_DIM), (0.25 * TOKEN_LENGTH ** 0.5), 48.0, ((0, 4), (2, 2)), jnp.float32)
    init_normalizer = gaussian(streams_of[10], (SEQUENCE_COUNT, 2, MEMORY_HEADS, HEAD_DIM), (0.25 * TOKEN_LENGTH ** 0.5), 48.0, ((0, 4), (2, 2)), jnp.float32)
    head_gain = jnp.clip(1.0 + 0.18 * jax.random.normal(streams_of[11], (MEMORY_HEADS, HEAD_DIM), jnp.float32), 0.1, 1.9)
    pool_weight = gaussian(streams_of[12], (D, D), D ** -0.5, 0.125, ((0, 16), (1, 2)))
    mem_out_weight = gaussian(streams_of[13], (D, MEM_W), MEM_W ** -0.5, 0.1875, ((0, 16), (1, 2)))
    pool_out_weight = gaussian(streams_of[14], (D, D), D ** -0.5, 0.125, ((0, 16), (1, 2)))
    return dict(tokens=tokens, norm_gain=norm_gain, query_weight=query_weight, key_weight=key_weight, value_weight=value_weight, outgate_weight=outgate_weight, gate_weight=gate_weight, gate_bias=gate_bias, decay_extra=decay_extra, init_memory=init_memory, init_normalizer=init_normalizer, head_gain=head_gain, pool_weight=pool_weight, mem_out_weight=mem_out_weight, pool_out_weight=pool_out_weight)


norm_eps = 1e-06
exact_mode = lax.Precision.HIGHEST

def block_output(query_rows, key_rows, value_rows, input_gate, log_forget, memory, normalizer, stabilizer):
    block_len = query_rows.shape[1]
    key_scale = key_rows.shape[-1] ** (-0.5)
    lower_mask = jnp.tril(jnp.ones((block_len, block_len), dtype=bool))
    summed = jnp.cumsum(log_forget, axis=-1)
    log_decay = jnp.where(lower_mask, summed[:, :, None] - summed[:, None, :] + input_gate[:, None, :], -jnp.inf)
    log_carry = stabilizer[:, None] + summed
    running_max = jnp.maximum(log_carry, lax.optimization_barrier(jnp.max(log_decay, axis=-1)))
    query_wide = query_rows.astype(jnp.float32)
    scores = jnp.einsum('btd,bsd->bts', query_wide, key_rows.astype(jnp.float32), precision=exact_mode) * key_scale
    inner_weight = jnp.exp(log_decay - running_max[:, :, None]) * scores
    weight_rounded = lax.optimization_barrier(inner_weight.astype(jnp.bfloat16))
    carry_weight = jnp.exp(log_carry - running_max)
    numerator = carry_weight[:, :, None] * jnp.einsum('bed,btd->bte', memory, query_wide, precision=exact_mode)
    numerator = numerator + jnp.einsum('bts,bse->bte', weight_rounded.astype(jnp.float32), value_rows.astype(jnp.float32), precision=exact_mode)
    denominator = carry_weight * jnp.einsum('bd,btd->bt', normalizer, query_wide, precision=exact_mode)
    denominator = denominator + lax.optimization_barrier(jnp.sum(inner_weight, axis=-1))
    return numerator / jnp.maximum(jnp.abs(denominator), jnp.exp(-running_max))[:, :, None]

def block_summary(key_rows, value_rows, input_gate, log_forget):
    key_wide = key_rows.astype(jnp.float32) * key_rows.shape[-1] ** (-0.5)
    summed = jnp.cumsum(log_forget, axis=-1)
    forget_total = summed[:, -1]
    log_weight = forget_total[:, None] - summed + input_gate
    running_max = lax.optimization_barrier(jnp.max(log_weight, axis=-1))
    weights = jnp.exp(log_weight - running_max[:, None])
    memory = jnp.einsum('bse,bsd->bed', weights[:, :, None] * value_rows.astype(jnp.float32), key_wide, precision=exact_mode)
    normalizer = jnp.einsum('bs,bsd->bd', weights, key_wide, precision=exact_mode)
    return (memory, normalizer, running_max, forget_total)

def combine(earlier, latter):
    early_memory, early_norm, early_max, early_total = earlier
    late_memory, late_norm, late_max, late_total = latter
    joint_max = jnp.maximum(early_max + late_total, late_max)
    early_scale = jnp.exp(early_max + late_total - joint_max)
    late_scale = jnp.exp(late_max - joint_max)
    memory = early_scale[:, None, None] * early_memory + late_scale[:, None, None] * late_memory
    normalizer = early_scale[:, None] * early_norm + late_scale[:, None] * late_norm
    return (memory, normalizer, joint_max, early_total + late_total)

def span_sweep(query_rows, key_rows, value_rows, input_gate, log_forget, memory, normalizer, stabilizer, span):
    block_count = query_rows.shape[1] // span

    def to_blocks(array):
        shaped = array.reshape((array.shape[0], block_count, span) + array.shape[2:])
        return jnp.moveaxis(shaped, 1, 0)

    def advance(carried, pieces):
        query_blk, key_blk, value_blk, gate_blk, forget_blk = pieces
        result = block_output(query_blk, key_blk, value_blk, gate_blk, forget_blk, carried[0], carried[1], carried[2])
        return (combine(carried, block_summary(key_blk, value_blk, gate_blk, forget_blk)), result)
    initial = (memory, normalizer, stabilizer, jnp.zeros_like(stabilizer))
    ignored, outputs = lax.scan(advance, initial, tuple((to_blocks(array) for array in (query_rows, key_rows, value_rows, input_gate, log_forget))))
    return jnp.moveaxis(outputs, 0, 1).reshape(query_rows.shape[:2] + (value_rows.shape[2],))

def direction_sweep(query_rows, key_rows, value_rows, input_gate, log_forget, memory, normalizer):
    zero_rows = jnp.zeros((memory.shape[0],), jnp.float32)
    return span_sweep(query_rows, key_rows, value_rows, input_gate, log_forget, memory, normalizer, zero_rows, math.gcd(T_DEV, 256))

def reverse_time(array):
    return jnp.flip(array, axis=1)

def pool_window(padded, positions, channels, seq_len, group_size):
    row_count = positions.shape[0]
    group_index = channels // group_size
    reach_left = jnp.left_shift(jnp.ones_like(group_index), group_index)
    reach_right = reach_left - 1
    window_sum = jnp.zeros((row_count, channels.shape[0]), jnp.float32)
    for offset in range(-HALO, HALO):
        inside = ((offset >= -reach_left) & (offset <= reach_right)).astype(jnp.float32)
        window_sum = window_sum + inside * padded[HALO + offset:HALO + offset + row_count]
    first_pos = jnp.maximum(positions[:, None] - reach_left[None, :], 0)
    last_pos = jnp.minimum(positions[:, None] + reach_right[None, :], seq_len - 1)
    counted = (last_pos - first_pos + 1).astype(jnp.float32)
    centre = padded[HALO:HALO + row_count]
    return (window_sum / counted - centre).astype(jnp.bfloat16)

def output_project(memory_out, pool_out, mem_out_weight, pool_out_weight):
    row_count = memory_out.shape[0]
    model_width = pool_out.shape[1]

    def grouped(matrix):
        return jnp.moveaxis(matrix.reshape(matrix.shape[0], N_TP, matrix.shape[1] // N_TP), 1, 0)

    def accumulate(running, pieces):
        mem_rows, pool_rows, mem_cols, pool_cols = pieces
        group_sum = lax.dot_general(mem_rows, mem_cols, (((1,), (1,)), ((), ())), preferred_element_type=jnp.float32)
        group_sum = group_sum + lax.dot_general(pool_rows, pool_cols, (((1,), (1,)), ((), ())), preferred_element_type=jnp.float32)
        rounded = lax.optimization_barrier(group_sum.astype(jnp.bfloat16))
        return (running + rounded.astype(jnp.float32), None)
    running, ignored = lax.scan(accumulate, jnp.zeros((row_count, model_width), jnp.float32), (grouped(memory_out), grouped(pool_out), grouped(mem_out_weight), grouped(pool_out_weight)))
    return running.astype(jnp.bfloat16)

def reference(tokens, norm_gain, query_weight, key_weight, value_weight, outgate_weight, gate_weight, gate_bias, decay_extra, init_memory, init_normalizer, head_gain, pool_weight, mem_out_weight, pool_out_weight):
    seq_count, seq_len, model_width = tokens.shape
    head_count, head_width = head_gain.shape
    flattened = tokens.reshape(seq_count * seq_len, model_width).astype(jnp.float32)
    normed = (flattened * lax.rsqrt(lax.optimization_barrier(jnp.mean(flattened * flattened, axis=-1, keepdims=True)) + norm_eps) * norm_gain).astype(jnp.bfloat16)

    def project(weight):
        return jnp.dot(normed, weight, preferred_element_type=jnp.float32).astype(jnp.bfloat16)
    query_proj = project(query_weight)
    key_proj = project(key_weight)
    value_proj = project(value_weight)
    outgate = project(outgate_weight)
    pool_input = project(pool_weight)
    gate_pre = lax.dot_general(normed, gate_weight.reshape(4 * head_count, model_width), (((1,), (1,)), ((), ())), preferred_element_type=jnp.float32) + gate_bias.reshape(4 * head_count)
    gate_pre = gate_pre.reshape(seq_count, seq_len, 4, head_count).transpose(2, 0, 3, 1).reshape(4, seq_count * head_count, seq_len)

    def to_heads(matrix):
        shaped = matrix.reshape(seq_count, seq_len, head_count, head_width).transpose(0, 2, 1, 3)
        return shaped.reshape(seq_count * head_count, seq_len, head_width)
    query_heads = to_heads(query_proj)
    key_heads = to_heads(key_proj)
    value_heads = to_heads(value_proj)
    extra_decay = decay_extra.transpose(1, 0, 2, 3).reshape(2, seq_count * head_count, seq_len)
    forward_forget = jax.nn.log_sigmoid(gate_pre[1]) + extra_decay[0]
    backward_forget = jax.nn.log_sigmoid(gate_pre[3]) + extra_decay[1]
    start_memory = init_memory.reshape(seq_count, 2, head_count, head_width, head_width)
    start_norm = init_normalizer.reshape(seq_count, 2, head_count, head_width)
    forward = direction_sweep(query_heads, key_heads, value_heads, gate_pre[0], forward_forget, start_memory[:, 0].reshape(-1, head_width, head_width), start_norm[:, 0].reshape(-1, head_width))
    backward = reverse_time(direction_sweep(reverse_time(query_heads), reverse_time(key_heads), reverse_time(value_heads), reverse_time(gate_pre[2]), reverse_time(backward_forget), start_memory[:, 1].reshape(-1, head_width, head_width), start_norm[:, 1].reshape(-1, head_width)))
    summed_dirs = (forward + backward).reshape(seq_count, head_count, seq_len, head_width).transpose(0, 2, 1, 3)
    summed_dirs = summed_dirs.reshape(seq_count * seq_len, head_count, head_width)
    normed_heads = summed_dirs * lax.rsqrt(lax.optimization_barrier(jnp.mean(summed_dirs * summed_dirs, axis=-1, keepdims=True)) + norm_eps) * head_gain
    out_gate = jax.nn.sigmoid(outgate.astype(jnp.float32).reshape(seq_count * seq_len, head_count, head_width))
    memory_out = (normed_heads * out_gate).astype(jnp.bfloat16).reshape(seq_count * seq_len, head_count * head_width)
    padded = jnp.pad(pool_input.reshape(seq_count, seq_len, model_width).astype(jnp.float32), ((0, 0), (HALO, HALO), (0, 0)))
    window_fn = partial(pool_window, positions=jnp.arange(seq_len, dtype=jnp.int32), channels=jnp.arange(model_width, dtype=jnp.int32), seq_len=seq_len, group_size=model_width // 4)
    pool_out = jax.vmap(window_fn)(padded).reshape(seq_count * seq_len, model_width)
    mixed = output_project(memory_out, pool_out, mem_out_weight, pool_out_weight)
    return mixed.reshape(seq_count, seq_len, model_width)
```

```python
import functools
import math

import jax
import jax.numpy as jnp
from jax import lax
from jax.experimental import pallas as pl
from jax.experimental.pallas import tpu as pltpu
from jax.sharding import PartitionSpec as P

MESH = pl.DeviceIdType.MESH

HALO = 8


norm_eps = 1e-06
exact_mode = lax.Precision.HIGHEST


def carried_in(x, axis, combine, identity, reverse):
    length, position = (lax.axis_size(axis), lax.axis_index(axis))
    everything = jax.tree.map(lambda part: lax.all_gather(part, axis), x)
    start = jax.tree.map(
        lambda part, zero: jnp.broadcast_to(jnp.asarray(zero, part.dtype), part.shape), x, identity
    )

    def lap(k, before):
        at = length - 1 - k if reverse else k
        reached = at > position if reverse else at < position
        new = combine(before, jax.tree.map(lambda part: part[at], everything))
        return jax.tree.map(lambda a, b: jnp.where(reached, a, b), new, before)

    return lax.fori_loop(0, length, lap, start)


def padded_2(block, sides, width):
    for axis, dim in sides:
        count = lax.axis_size(axis)
        forward = [(i, i + 1) for i in range(count - 1)]
        backward = [(target, source) for source, target in forward]
        low = lax.ppermute(
            lax.slice_in_dim(block, block.shape[dim] - width, None, axis=dim), axis, forward
        )
        high = lax.ppermute(lax.slice_in_dim(block, 0, width, axis=dim), axis, backward)
        block = jnp.concatenate([low, block, high], axis=dim)
    return block


def block_output(
    query_rows, key_rows, value_rows, input_gate, log_forget, memory, normalizer, stabilizer
):
    block_len = query_rows.shape[1]
    key_scale = key_rows.shape[-1] ** (-0.5)
    lower_mask = jnp.tril(jnp.ones((block_len, block_len), dtype=bool))
    summed = jnp.cumsum(log_forget, axis=-1)
    log_decay = jnp.where(
        lower_mask, summed[:, :, None] - summed[:, None, :] + input_gate[:, None, :], -jnp.inf
    )
    log_carry = stabilizer[:, None] + summed
    running_max = jnp.maximum(log_carry, jnp.max(log_decay, axis=-1))
    scores = (
        jnp.einsum("btd,bsd->bts", query_rows, key_rows, preferred_element_type=jnp.float32)
        * key_scale
    )
    inner_weight = jnp.exp(log_decay - running_max[:, :, None]) * scores
    weight_rounded = inner_weight.astype(jnp.bfloat16)
    carry_weight = jnp.exp(log_carry - running_max)
    query_wide = query_rows.astype(jnp.float32)
    numerator = carry_weight[:, :, None] * jnp.einsum(
        "bed,btd->bte", memory, query_wide, precision=exact_mode
    )
    numerator = numerator + jnp.einsum(
        "bts,bse->bte", weight_rounded, value_rows, preferred_element_type=jnp.float32
    )
    denominator = carry_weight * jnp.einsum(
        "bd,btd->bt", normalizer, query_wide, precision=exact_mode
    )
    denominator = denominator + jnp.sum(inner_weight, axis=-1)
    return numerator / jnp.maximum(jnp.abs(denominator), jnp.exp(-running_max))[:, :, None]


def block_summary(key_rows, value_rows, input_gate, log_forget):
    key_wide = key_rows.astype(jnp.float32) * key_rows.shape[-1] ** (-0.5)
    summed = jnp.cumsum(log_forget, axis=-1)
    forget_total = summed[:, -1]
    log_weight = forget_total[:, None] - summed + input_gate
    running_max = jnp.max(log_weight, axis=-1)
    weights = jnp.exp(log_weight - running_max[:, None])
    memory = jnp.einsum(
        "bse,bsd->bed",
        weights[:, :, None] * value_rows.astype(jnp.float32),
        key_wide,
        precision=exact_mode,
    )
    normalizer = jnp.einsum("bs,bsd->bd", weights, key_wide, precision=exact_mode)
    return (memory, normalizer, running_max, forget_total)


def combine(earlier, latter):
    early_memory, early_norm, early_max, early_total = earlier
    late_memory, late_norm, late_max, late_total = latter
    joint_max = jnp.maximum(early_max + late_total, late_max)
    early_scale = jnp.exp(early_max + late_total - joint_max)
    late_scale = jnp.exp(late_max - joint_max)
    memory = early_scale[:, None, None] * early_memory + late_scale[:, None, None] * late_memory
    normalizer = early_scale[:, None] * early_norm + late_scale[:, None] * late_norm
    return (memory, normalizer, joint_max, early_total + late_total)


def span_sweep(
    query_rows, key_rows, value_rows, input_gate, log_forget, memory, normalizer, stabilizer, span
):
    block_count = query_rows.shape[1] // span

    def to_blocks(array):
        shaped = array.reshape((array.shape[0], block_count, span) + array.shape[2:])
        return jnp.moveaxis(shaped, 1, 0)

    def advance(carried, pieces):
        query_blk, key_blk, value_blk, gate_blk, forget_blk = pieces
        result = block_output(
            query_blk, key_blk, value_blk, gate_blk, forget_blk, carried[0], carried[1], carried[2]
        )
        return (combine(carried, block_summary(key_blk, value_blk, gate_blk, forget_blk)), result)

    initial = (memory, normalizer, stabilizer, jnp.zeros_like(stabilizer))
    ignored, outputs = lax.scan(
        advance,
        initial,
        tuple(
            (
                to_blocks(array)
                for array in (query_rows, key_rows, value_rows, input_gate, log_forget)
            )
        ),
    )
    return jnp.moveaxis(outputs, 0, 1).reshape(query_rows.shape[:2] + (value_rows.shape[2],))


def reverse_time(array):
    return jnp.flip(array, axis=1)


def to_heads(matrix, head_count):
    shaped = matrix.reshape(matrix.shape[0], head_count, matrix.shape[1] // head_count)
    return shaped.transpose(1, 0, 2)


def pool_window(padded, positions, channels, seq_len, group_size):
    row_count = positions.shape[0]
    group_index = channels // group_size
    reach_left = jnp.left_shift(jnp.ones_like(group_index), group_index)
    reach_right = reach_left - 1
    window_sum = jnp.zeros((row_count, channels.shape[0]), jnp.float32)
    for offset in range(-HALO, HALO):
        inside = ((offset >= -reach_left) & (offset <= reach_right)).astype(jnp.float32)
        window_sum = window_sum + inside * padded[HALO + offset : HALO + offset + row_count]
    first_pos = jnp.maximum(positions[:, None] - reach_left[None, :], 0)
    last_pos = jnp.minimum(positions[:, None] + reach_right[None, :], seq_len - 1)
    counted = (last_pos - first_pos + 1).astype(jnp.float32)
    centre = padded[HALO : HALO + row_count]
    return (window_sum / counted - centre).astype(jnp.bfloat16)


def per_device(
    tokens,
    norm_gain,
    query_weight,
    key_weight,
    value_weight,
    outgate_weight,
    gate_weight,
    gate_bias,
    decay_extra,
    init_memory,
    init_normalizer,
    head_gain,
    pool_weight,
    mem_out_weight,
    pool_out_weight,
):
    block_len = tokens.shape[1]
    model_width = tokens.shape[2]
    head_count, head_width = head_gain.shape
    span = math.gcd(block_len, 256)
    flattened = tokens[0].astype(jnp.float32)
    normed = (
        flattened
        * lax.rsqrt(jnp.mean(flattened * flattened, axis=-1, keepdims=True) + norm_eps)
        * norm_gain
    ).astype(jnp.bfloat16)
    zero_start = tuple(
        (
            jnp.zeros((block_len, weight.shape[1]), jnp.float32)
            for weight in (query_weight, key_weight, value_weight, outgate_weight, pool_weight)
        )
    )
    zero_start = zero_start + (
        jnp.zeros((model_width, mem_out_weight.shape[1]), jnp.bfloat16),
        jnp.zeros((model_width, pool_out_weight.shape[1]), jnp.bfloat16),
    )
    line_query, line_key, line_value, line_outgate, line_pool, line_mem_out, line_pool_out = (
        lax.all_gather(query_weight, "fs", axis=0, tiled=True),
        lax.all_gather(key_weight, "fs", axis=0, tiled=True),
        lax.all_gather(value_weight, "fs", axis=0, tiled=True),
        lax.all_gather(outgate_weight, "fs", axis=0, tiled=True),
        lax.all_gather(pool_weight, "fs", axis=0, tiled=True),
        lax.all_gather(mem_out_weight, "fs", axis=0, tiled=True),
        lax.all_gather(pool_out_weight, "fs", axis=0, tiled=True),
    )
    pieces = (
        lax.all_gather(line_query, "sp", axis=0, tiled=True),
        lax.all_gather(line_key, "sp", axis=0, tiled=True),
        lax.all_gather(line_value, "sp", axis=0, tiled=True),
        lax.all_gather(line_outgate, "sp", axis=0, tiled=True),
        lax.all_gather(line_pool, "sp", axis=0, tiled=True),
        lax.all_gather(line_mem_out, "sp", axis=0, tiled=True),
        lax.all_gather(line_pool_out, "sp", axis=0, tiled=True),
    )
    partial_sums = tuple(
        (
            jnp.dot(normed, weight_rows, preferred_element_type=jnp.float32)
            for weight_rows in pieces[:5]
        )
    )
    collected = tuple((weight_rows for weight_rows in pieces[5:]))
    folded = partial_sums + collected
    query_proj, key_proj, value_proj, outgate, pool_input = tuple(
        (running.astype(jnp.bfloat16) for running in folded[:5])
    )
    mem_weight_all = folded[5]
    pool_weight_all = folded[6]
    gate_pre = lax.dot_general(
        normed,
        gate_weight.reshape(4 * head_count, model_width),
        (((1,), (1,)), ((), ())),
        preferred_element_type=jnp.float32,
    ) + gate_bias.reshape(4 * head_count)
    gate_pre = gate_pre.reshape(block_len, 4, head_count).transpose(1, 2, 0)
    query_heads = to_heads(query_proj, head_count)
    key_heads = to_heads(key_proj, head_count)
    value_heads = to_heads(value_proj, head_count)
    forward_forget = jax.nn.log_sigmoid(gate_pre[1]) + decay_extra[0, 0]
    backward_forget = jax.nn.log_sigmoid(gate_pre[3]) + decay_extra[0, 1]
    zero_rows = jnp.zeros((head_count,), jnp.float32)
    identity = (
        jnp.zeros((head_count, head_width, head_width), jnp.float32),
        jnp.zeros((head_count, head_width), jnp.float32),
        jnp.full((head_count,), -1e30, jnp.float32),
        zero_rows,
    )
    front_memory, front_norm, front_max, front_total = block_summary(
        key_heads, value_heads, gate_pre[0], forward_forget
    )
    prefix = carried_in(
        (front_memory, front_norm, front_max, front_total), "sp", combine, identity, False
    )
    incoming = combine((init_memory[0, 0], init_normalizer[0, 0], zero_rows, zero_rows), prefix)
    forward_out = span_sweep(
        query_heads,
        key_heads,
        value_heads,
        gate_pre[0],
        forward_forget,
        incoming[0],
        incoming[1],
        incoming[2],
        span,
    )
    back_query = reverse_time(query_heads)
    back_key = reverse_time(key_heads)
    back_value = reverse_time(value_heads)
    back_gate = reverse_time(gate_pre[2])
    back_forget = reverse_time(backward_forget)
    rear_memory, rear_norm, rear_max, rear_total = block_summary(
        back_key, back_value, back_gate, back_forget
    )
    suffix = carried_in(
        (rear_memory, rear_norm, rear_max, rear_total), "sp", combine, identity, True
    )
    back_incoming = combine(
        (init_memory[0, 1], init_normalizer[0, 1], zero_rows, zero_rows), suffix
    )
    backward_out = reverse_time(
        span_sweep(
            back_query,
            back_key,
            back_value,
            back_gate,
            back_forget,
            back_incoming[0],
            back_incoming[1],
            back_incoming[2],
            span,
        )
    )
    summed_dirs = (forward_out + backward_out).transpose(1, 0, 2)
    normed_heads = (
        summed_dirs
        * lax.rsqrt(jnp.mean(summed_dirs * summed_dirs, axis=-1, keepdims=True) + norm_eps)
        * head_gain
    )
    out_gate = jax.nn.sigmoid(
        outgate.astype(jnp.float32).reshape(block_len, head_count, head_width)
    )
    memory_out = (
        (normed_heads * out_gate).astype(jnp.bfloat16).reshape(block_len, head_count * head_width)
    )
    padded = padded_2(pool_input, (("sp", 0),), HALO).astype(jnp.float32)
    feature_count = pool_input.shape[1]
    positions = lax.axis_index("sp") * block_len + jnp.arange(block_len, dtype=jnp.int32)
    channels = lax.axis_index("tp") * feature_count + jnp.arange(feature_count, dtype=jnp.int32)
    pool_out = pool_window(
        padded, positions, channels, block_len * lax.axis_size("sp"), model_width // 4
    )
    own_rows = block_len // lax.axis_size("tp")
    result = lax.dot_general(
        memory_out, mem_weight_all, (((1,), (1,)), ((), ())), preferred_element_type=jnp.float32
    )
    mixed = lax.psum_scatter(
        (
            result
            + lax.dot_general(
                pool_out,
                pool_weight_all,
                (((1,), (1,)), ((), ())),
                preferred_element_type=jnp.float32,
            )
        ).astype(jnp.bfloat16),
        "tp",
        scatter_dimension=0,
        tiled=True,
    )
    return mixed.reshape(1, own_rows, model_width)


def aligned(start, size):
    return pl.ds(pl.multiple_of(start, size), size)


def gather_kernel(n_sp, n_fs, widths, *refs):
    count = len(widths)
    token_ref, decay_ref = refs[:2]
    weight_refs = refs[2 : 2 + count]
    x_ref, decay_out, in_ref, out_ref = refs[2 + count : 6 + count]
    (
        local_sem,
        token_local,
        weight_send,
        weight_recv,
        decay_send,
        decay_recv,
        token_send,
        token_recv,
        swap_send,
        swap_recv,
        row_send,
        row_recv,
    ) = refs[6 + count :]
    sp, fs, tp = (lax.axis_index(name) for name in ("sp", "fs", "tp"))
    other = 1 - tp
    rows = weight_refs[0].shape[0]
    block = token_ref.shape[0]
    half = block // 2
    ups = [lax.rem(sp + k, n_sp) for k in range(n_sp)]
    downs = [lax.rem(sp + n_sp - k, n_sp) for k in range(n_sp)]
    fs_up = [lax.rem(fs + j, n_fs) for j in range(n_fs)]
    fs_down = [lax.rem(fs + n_fs - j, n_fs) for j in range(n_fs)]

    barrier = pltpu.get_barrier_semaphore()
    for k in range(1, n_sp):
        pl.semaphore_signal(barrier, inc=1, device_id={"sp": ups[k]}, device_id_type=MESH)
    for j in range(1, n_fs):
        pl.semaphore_signal(barrier, inc=1, device_id={"fs": fs_up[j]}, device_id_type=MESH)
    pl.semaphore_signal(barrier, inc=1, device_id={"tp": other}, device_id_type=MESH)
    pl.semaphore_wait(barrier, n_sp + n_fs - 1)

    in_count = count - 2
    in_width = sum(widths[:in_count])

    def landing(i, source_sp):
        at = aligned((source_sp * n_fs + fs) * rows, rows)
        start = sum(widths[:i])
        if i < in_count:
            return in_ref.at[at, pl.ds(start, widths[i])]
        return out_ref.at[at, pl.ds(start - in_width, widths[i])]

    def piece(i, target_sp):
        return weight_refs[i].at[:, aligned(target_sp * widths[i], widths[i])]

    locals_ = []
    for i in range(count):
        locals_.append(pltpu.make_async_copy(piece(i, sp), landing(i, sp), local_sem.at[i]))
    for copy in locals_:
        copy.start()
    own_tokens = pltpu.make_async_copy(
        token_ref, x_ref.at[aligned(sp * block, block)], token_local.at[0]
    )
    own_tokens.start()
    own_decay = pltpu.make_async_copy(decay_ref.at[sp], decay_out.at[sp], token_local.at[1])
    own_decay.start()

    def weight_copy(i, k, target, source):
        return pltpu.make_async_remote_copy(
            src_ref=piece(i, target),
            dst_ref=landing(i, source),
            send_sem=weight_send.at[k - 1, i],
            recv_sem=weight_recv.at[k - 1, i],
            device_id={"sp": target},
            device_id_type=MESH,
        )

    def decay_copy(k, target, source):
        return pltpu.make_async_remote_copy(
            src_ref=decay_ref.at[target],
            dst_ref=decay_out.at[source],
            send_sem=decay_send.at[k - 1],
            recv_sem=decay_recv.at[k - 1],
            device_id={"sp": target},
            device_id_type=MESH,
        )

    def token_copy(k, target, source):
        return pltpu.make_async_remote_copy(
            src_ref=token_ref.at[aligned(tp * half, half)],
            dst_ref=x_ref.at[aligned(source * block + tp * half, half)],
            send_sem=token_send.at[k - 1],
            recv_sem=token_recv.at[k - 1],
            device_id={"sp": target},
            device_id_type=MESH,
        )

    def swap_copy(k, side):
        at = x_ref.at[aligned(downs[k] * block + side * half, half)]
        return pltpu.make_async_remote_copy(
            src_ref=at,
            dst_ref=at,
            send_sem=swap_send.at[k - 1],
            recv_sem=swap_recv.at[k - 1],
            device_id={"tp": other},
            device_id_type=MESH,
        )

    def row_copies(k, j, at_fs):
        at = aligned((downs[k] * n_fs + at_fs) * rows, rows)
        made = []
        for which, ref in enumerate((in_ref, out_ref)):
            made.append(
                pltpu.make_async_remote_copy(
                    src_ref=ref.at[at],
                    dst_ref=ref.at[at],
                    send_sem=row_send.at[k, j - 1, which],
                    recv_sem=row_recv.at[k, j - 1, which],
                    device_id={"fs": fs_up[j]},
                    device_id_type=MESH,
                )
            )
        return made

    for k in range(1, n_sp):
        for i in range(count):
            weight_copy(i, k, ups[k], sp).start()
    for k in range(1, n_sp):
        decay_copy(k, ups[k], sp).start()
        token_copy(k, ups[k], sp).start()
    for copy in locals_:
        copy.wait()
    for k in range(n_sp):
        if k:
            for i in range(count):
                weight_copy(i, k, ups[k], downs[k]).wait_recv()
        for j in range(1, n_fs):
            for copy in row_copies(k, j, fs):
                copy.start()
    for k in range(1, n_sp):
        token_copy(k, ups[k], downs[k]).wait_recv()
        swap_copy(k, tp).start()
    own_tokens.wait()
    own_decay.wait()
    for k in range(1, n_sp):
        decay_copy(k, ups[k], downs[k]).wait_recv()
        swap_copy(k, other).wait_recv()
    for k in range(n_sp):
        for j in range(1, n_fs):
            for copy in row_copies(k, j, fs_down[j]):
                copy.wait_recv()
    for k in range(1, n_sp):
        for i in range(count):
            weight_copy(i, k, ups[k], sp).wait_send()
        decay_copy(k, ups[k], sp).wait_send()
        token_copy(k, ups[k], sp).wait_send()
        swap_copy(k, tp).wait_send()
    for k in range(n_sp):
        for j in range(1, n_fs):
            for copy in row_copies(k, j, fs):
                copy.wait_send()


def gather_all(tokens, decay, weights):
    n_sp, n_fs = lax.axis_size("sp"), lax.axis_size("fs")
    widths = tuple(weight.shape[1] // n_sp for weight in weights)
    block, model_width = tokens.shape
    count = len(weights)
    vmem = pl.BlockSpec(memory_space=pltpu.VMEM)
    dma = pltpu.SemaphoreType.DMA
    return pl.pallas_call(
        functools.partial(gather_kernel, n_sp, n_fs, widths),
        out_shape=(
            jax.ShapeDtypeStruct((n_sp * block, model_width), tokens.dtype),
            jax.ShapeDtypeStruct(decay.shape, decay.dtype),
            jax.ShapeDtypeStruct((model_width, sum(widths[:-2])), tokens.dtype),
            jax.ShapeDtypeStruct((model_width, sum(widths[-2:])), tokens.dtype),
        ),
        in_specs=[vmem] * (2 + count),
        out_specs=(vmem,) * 4,
        scratch_shapes=[
            dma((count,)),
            dma((2,)),
            dma((n_sp - 1, count)),
            dma((n_sp - 1, count)),
            dma((n_sp - 1,)),
            dma((n_sp - 1,)),
            dma((n_sp - 1,)),
            dma((n_sp - 1,)),
            dma((n_sp - 1,)),
            dma((n_sp - 1,)),
            dma((n_sp, n_fs - 1, 2)),
            dma((n_sp, n_fs - 1, 2)),
        ],
        compiler_params=pltpu.CompilerParams(
            collective_id=0, has_side_effects=True, vmem_limit_bytes=40 * 2**20
        ),
        name="gather_all",
    )(tokens, decay, *weights)


def memory_kernel(
    q_ref, qk_ref, k_ref, v_ref, gate_ref, cols_ref, rows_ref, mem_ref, norm_ref, gain_ref, o_ref
):
    tb = q_ref.shape[0]
    seq = k_ref.shape[0]
    width = q_ref.shape[1]
    scale = width ** (-0.5)
    q = q_ref[...]
    cols = cols_ref[...]
    front_peak, rear_peak = cols[:, 0:1], cols[:, 1:2]
    front_max, rear_max = cols[:, 2:3], cols[:, 3:4]
    rear_own = cols[:, 4:5]
    score = (
        lax.dot_general(
            q, k_ref[...], (((1,), (1,)), ((), ())), preferred_element_type=jnp.float32
        )
        * scale
    )
    t = pl.program_id(0) * tb + lax.broadcasted_iota(jnp.int32, (tb, seq), 0)
    s = lax.broadcasted_iota(jnp.int32, (tb, seq), 1)
    front = s <= t
    weight = (
        jnp.exp(
            jnp.where(front, rows_ref[0:1, :] - front_peak, rows_ref[1:2, :] - rear_peak)
        )
        * score
    )
    front_weight = jnp.where(front, weight, 0.0)
    rear_weight = jnp.where(front, 0.0, weight)
    wide = q.astype(jnp.float32)
    own_score = jnp.sum(wide * qk_ref[...].astype(jnp.float32), axis=1, keepdims=True) * scale
    own_weight = jnp.exp(rear_own - rear_peak) * own_score
    start = t.shape[0] * pl.program_id(0)
    own_value = v_ref[pl.ds(pl.multiple_of(start, tb), tb), :].astype(jnp.float32)
    carry = lax.dot_general(
        wide,
        mem_ref[...],
        (((1,), (1,)), ((), ())),
        precision=exact_mode,
        preferred_element_type=jnp.float32,
    )

    def one(direction, weights, peak, top, extra_num, extra_den):
        decay = jnp.exp(-peak)
        num = decay * carry[:, direction * width : (direction + 1) * width] + jnp.dot(
            weights.astype(jnp.bfloat16), v_ref[...], preferred_element_type=jnp.float32
        )
        den = decay * jnp.sum(
            wide * norm_ref[direction : direction + 1, :], axis=1, keepdims=True
        ) + jnp.sum(weights, axis=1, keepdims=True)
        return (num + extra_num) / jnp.maximum(jnp.abs(den + extra_den), jnp.exp(-top))

    total = one(0, front_weight, front_peak, front_max, 0.0, 0.0) + one(
        1,
        rear_weight,
        rear_peak,
        rear_max,
        own_weight.astype(jnp.bfloat16).astype(jnp.float32) * own_value,
        own_weight,
    )
    normed = (
        total
        * lax.rsqrt(jnp.mean(total * total, axis=-1, keepdims=True) + norm_eps)
        * gain_ref[...]
    )
    o_ref[...] = (normed * jax.nn.sigmoid(gate_ref[...].astype(jnp.float32))).astype(jnp.bfloat16)


def memory_mix(proj, cols, rows, memory, normalizer, gain, width):
    seq = proj.shape[0]
    tb = math.gcd(seq, 256)

    def part(i, whole):
        if whole:
            return pl.BlockSpec((seq, width), lambda t: (0, i))
        return pl.BlockSpec((tb, width), lambda t: (t, i))

    def fixed(array):
        return pl.BlockSpec(array.shape, lambda t: (0, 0))

    return pl.pallas_call(
        memory_kernel,
        grid=(seq // tb,),
        out_shape=jax.ShapeDtypeStruct((seq, width), jnp.bfloat16),
        in_specs=[
            part(0, False),
            part(1, False),
            part(1, True),
            part(2, True),
            part(3, False),
            pl.BlockSpec((tb, cols.shape[1]), lambda t: (t, 0)),
            fixed(rows),
            fixed(memory),
            fixed(normalizer),
            fixed(gain),
        ],
        out_specs=pl.BlockSpec((tb, width), lambda t: (t, 0)),
        name="memory_mix",
    )(proj, proj, proj, proj, proj, cols, rows, memory, normalizer, gain)


def project_kernel(
    n_sp, mem_ref, pool_ref, weight_ref, o_ref,
    give, take, send, land, own, swap_send, swap_recv, z_send, z_recv,
):
    sp, tp = lax.axis_index("sp"), lax.axis_index("tp")
    other = 1 - tp
    half = o_ref.shape[0]
    width = o_ref.shape[1]
    split = mem_ref.shape[1]
    tile = math.gcd(width, 512)

    barrier = pltpu.get_barrier_semaphore()
    for k in range(1, n_sp):
        pl.semaphore_signal(
            barrier, inc=1, device_id={"sp": lax.rem(sp + k, n_sp)}, device_id_type=MESH
        )
    pl.semaphore_signal(barrier, inc=1, device_id={"tp": other}, device_id_type=MESH)
    pl.semaphore_wait(barrier, n_sp)

    def product(target, side, c):
        at = aligned(target * 2 * half + side * half, half)
        columns = pl.ds(c * tile, tile)
        dims = (((1,), (1,)), ((), ()))
        return lax.dot_general(
            mem_ref[at, :],
            weight_ref[columns, :split],
            dims,
            preferred_element_type=jnp.float32,
        ) + lax.dot_general(
            pool_ref[at, :],
            weight_ref[columns, split:],
            dims,
            preferred_element_type=jnp.float32,
        )

    def swap(k):
        return pltpu.make_async_remote_copy(
            src_ref=give.at[k],
            dst_ref=take.at[k],
            send_sem=swap_send.at[k],
            recv_sem=swap_recv.at[k],
            device_id={"tp": other},
            device_id_type=MESH,
        )

    def pass_on(k):
        return pltpu.make_async_remote_copy(
            src_ref=send.at[k - 1],
            dst_ref=land.at[k - 1],
            send_sem=z_send.at[k - 1],
            recv_sem=z_recv.at[k - 1],
            device_id={"sp": lax.rem(sp + k, n_sp)},
            device_id_type=MESH,
        )

    order = list(range(1, n_sp)) + [0]
    for k in order:
        target = lax.rem(sp + k, n_sp)
        for c in range(width // tile):
            give[k, :, c * tile : (c + 1) * tile] = product(target, other, c).astype(jnp.bfloat16)
        swap(k).start()
    for k in order:
        target = lax.rem(sp + k, n_sp)
        swap(k).wait_recv()
        for c in range(width // tile):
            at = slice(c * tile, (c + 1) * tile)
            both = product(target, tp, c) + take[k, :, at].astype(jnp.float32)
            if k:
                send[k - 1, :, at] = both.astype(jnp.bfloat16)
            else:
                own[:, at] = both
        if k:
            pass_on(k).start()
    for k in range(1, n_sp):
        pass_on(k).wait_recv()
        own[...] += land[k - 1].astype(jnp.float32)
    o_ref[...] = own[...].astype(jnp.bfloat16)
    for k in range(n_sp):
        swap(k).wait_send()
        if k:
            pass_on(k).wait_send()


def project_out(memory_out, pool_out, weight):
    n_sp = lax.axis_size("sp")
    half = memory_out.shape[0] // (2 * n_sp)
    width = weight.shape[0]
    vmem = pl.BlockSpec(memory_space=pltpu.VMEM)
    dma = pltpu.SemaphoreType.DMA
    buffers = pltpu.VMEM((n_sp, half, width), jnp.bfloat16)
    fewer = pltpu.VMEM((n_sp - 1, half, width), jnp.bfloat16)
    return pl.pallas_call(
        functools.partial(project_kernel, n_sp),
        out_shape=jax.ShapeDtypeStruct((half, width), jnp.bfloat16),
        in_specs=[vmem] * 3,
        out_specs=vmem,
        scratch_shapes=[
            buffers,
            buffers,
            fewer,
            fewer,
            pltpu.VMEM((half, width), jnp.float32),
            dma((n_sp,)),
            dma((n_sp,)),
            dma((n_sp - 1,)),
            dma((n_sp - 1,)),
        ],
        compiler_params=pltpu.CompilerParams(
            collective_id=1, has_side_effects=True, vmem_limit_bytes=40 * 2**20
        ),
        name="project_out",
    )(memory_out, pool_out, weight)


def by_head(
    tokens,
    norm_gain,
    query_weight,
    key_weight,
    value_weight,
    outgate_weight,
    gate_weight,
    gate_bias,
    decay_extra,
    init_memory,
    init_normalizer,
    head_gain,
    pool_weight,
    mem_out_weight,
    pool_out_weight,
):
    model_width = tokens.shape[2]
    width = head_gain.shape[1]
    n_sp = lax.axis_size("sp")
    sp, tp = lax.axis_index("sp"), lax.axis_index("tp")
    everything, decay, in_weight, out_weight = gather_all(
        tokens[0],
        decay_extra[0].transpose(1, 0, 2),
        (
            query_weight,
            key_weight,
            value_weight,
            outgate_weight,
            pool_weight,
            mem_out_weight,
            pool_out_weight,
        ),
    )
    seq = everything.shape[0]
    decay = decay.transpose(1, 0, 2).reshape(2, seq)
    flattened = everything.astype(jnp.float32)
    normed = (
        flattened
        * lax.rsqrt(jnp.mean(flattened * flattened, axis=-1, keepdims=True) + norm_eps)
        * norm_gain
    ).astype(jnp.bfloat16)
    proj = jnp.dot(normed, in_weight, preferred_element_type=jnp.float32).astype(jnp.bfloat16)
    own_gates = lax.dynamic_index_in_dim(gate_weight, sp, 1, keepdims=False)
    own_bias = lax.dynamic_index_in_dim(gate_bias, sp, 1, keepdims=True)
    gate_pre = (
        lax.dot_general(
            own_gates, normed, (((1,), (1,)), ((), ())), preferred_element_type=jnp.float32
        )
        + own_bias
    )
    front_sum = lax.cumsum(jax.nn.log_sigmoid(gate_pre[1]) + decay[0])
    rear_sum = lax.cumsum(jax.nn.log_sigmoid(gate_pre[3]) + decay[1], reverse=True)
    front_level = gate_pre[0] - front_sum
    rear_level = gate_pre[2] - rear_sum
    front_peak = jnp.maximum(lax.cummax(front_level), 0.0)
    rear_peak = jnp.maximum(lax.cummax(rear_level, reverse=True), 0.0)
    rows = jnp.stack([front_level, rear_level])
    cols = jnp.stack(
        [front_peak, rear_peak, front_sum + front_peak, rear_sum + rear_peak, rear_level]
    ).T
    memory = lax.dynamic_index_in_dim(init_memory[0], sp, 1, keepdims=False)
    normalizer = lax.dynamic_index_in_dim(init_normalizer[0], sp, 1, keepdims=False)
    gain = lax.dynamic_slice_in_dim(head_gain, sp, 1, 0)
    memory_out = memory_mix(
        proj, cols, rows, memory.reshape(2 * width, width), normalizer, gain, width
    )
    pool_input = proj[:, 4 * width :]
    features = pool_input.shape[1]
    padded = jnp.pad(pool_input.astype(jnp.float32), ((HALO, HALO), (0, 0)))
    positions = jnp.arange(seq, dtype=jnp.int32)
    channels = (tp * n_sp + sp) * features + jnp.arange(features, dtype=jnp.int32)
    pool_out = pool_window(padded, positions, channels, seq, model_width // 4)
    mixed = project_out(memory_out, pool_out, out_weight)
    return mixed[None]


def solution(mesh):
    placed = (
        P("fs", "sp", None),
        P(),
        P(("sp", "fs"), "tp"),
        P(("sp", "fs"), "tp"),
        P(("sp", "fs"), "tp"),
        P(("sp", "fs"), "tp"),
        P(None, "tp", None),
        P(None, "tp"),
        P("fs", None, "tp", "sp"),
        P("fs", None, "tp", None, None),
        P("fs", None, "tp", None),
        P("tp", None),
        P(("sp", "fs"), "tp"),
        P(("sp", "fs"), "tp"),
        P(("sp", "fs"), "tp"),
    )

    def body(*args):
        heads, width = args[11].shape
        features = args[12].shape[1]
        fits = (
            lax.axis_size("tp") == 2
            and heads == lax.axis_size("sp")
            and heads > 1
            and lax.axis_size("fs") > 1
            and width == 128
            and features % (128 * heads) == 0
            and args[0].shape[1] % 32 == 0
        )
        return (by_head if fits else per_device)(*args)

    return jax.shard_map(
        body,
        mesh=mesh,
        in_specs=placed,
        out_specs=P("fs", ("sp", "tp"), None),
        check_vma=False,
    )
```

```python
import functools
import math

import jax
import jax.numpy as jnp
from jax import lax
from jax.experimental import pallas as pl
from jax.experimental.pallas import tpu as pltpu
from jax.sharding import PartitionSpec as P

MESH = pl.DeviceIdType.MESH

HALO = 8


norm_eps = 1e-06
exact_mode = lax.Precision.HIGHEST


def carried_in(x, axis, combine, identity, reverse):
    length, position = (lax.axis_size(axis), lax.axis_index(axis))
    everything = jax.tree.map(lambda part: lax.all_gather(part, axis), x)
    start = jax.tree.map(
        lambda part, zero: jnp.broadcast_to(jnp.asarray(zero, part.dtype), part.shape), x, identity
    )

    def lap(k, before):
        at = length - 1 - k if reverse else k
        reached = at > position if reverse else at < position
        new = combine(before, jax.tree.map(lambda part: part[at], everything))
        return jax.tree.map(lambda a, b: jnp.where(reached, a, b), new, before)

    return lax.fori_loop(0, length, lap, start)


def padded_2(block, sides, width):
    for axis, dim in sides:
        count = lax.axis_size(axis)
        forward = [(i, i + 1) for i in range(count - 1)]
        backward = [(target, source) for source, target in forward]
        low = lax.ppermute(
            lax.slice_in_dim(block, block.shape[dim] - width, None, axis=dim), axis, forward
        )
        high = lax.ppermute(lax.slice_in_dim(block, 0, width, axis=dim), axis, backward)
        block = jnp.concatenate([low, block, high], axis=dim)
    return block


def block_output(
    query_rows, key_rows, value_rows, input_gate, log_forget, memory, normalizer, stabilizer
):
    block_len = query_rows.shape[1]
    key_scale = key_rows.shape[-1] ** (-0.5)
    lower_mask = jnp.tril(jnp.ones((block_len, block_len), dtype=bool))
    summed = jnp.cumsum(log_forget, axis=-1)
    log_decay = jnp.where(
        lower_mask, summed[:, :, None] - summed[:, None, :] + input_gate[:, None, :], -jnp.inf
    )
    log_carry = stabilizer[:, None] + summed
    running_max = jnp.maximum(log_carry, jnp.max(log_decay, axis=-1))
    scores = (
        jnp.einsum("btd,bsd->bts", query_rows, key_rows, preferred_element_type=jnp.float32)
        * key_scale
    )
    inner_weight = jnp.exp(log_decay - running_max[:, :, None]) * scores
    weight_rounded = inner_weight.astype(jnp.bfloat16)
    carry_weight = jnp.exp(log_carry - running_max)
    query_wide = query_rows.astype(jnp.float32)
    numerator = carry_weight[:, :, None] * jnp.einsum(
        "bed,btd->bte", memory, query_wide, precision=exact_mode
    )
    numerator = numerator + jnp.einsum(
        "bts,bse->bte", weight_rounded, value_rows, preferred_element_type=jnp.float32
    )
    denominator = carry_weight * jnp.einsum(
        "bd,btd->bt", normalizer, query_wide, precision=exact_mode
    )
    denominator = denominator + jnp.sum(inner_weight, axis=-1)
    return numerator / jnp.maximum(jnp.abs(denominator), jnp.exp(-running_max))[:, :, None]


def block_summary(key_rows, value_rows, input_gate, log_forget):
    key_wide = key_rows.astype(jnp.float32) * key_rows.shape[-1] ** (-0.5)
    summed = jnp.cumsum(log_forget, axis=-1)
    forget_total = summed[:, -1]
    log_weight = forget_total[:, None] - summed + input_gate
    running_max = jnp.max(log_weight, axis=-1)
    weights = jnp.exp(log_weight - running_max[:, None])
    memory = jnp.einsum(
        "bse,bsd->bed",
        weights[:, :, None] * value_rows.astype(jnp.float32),
        key_wide,
        precision=exact_mode,
    )
    normalizer = jnp.einsum("bs,bsd->bd", weights, key_wide, precision=exact_mode)
    return (memory, normalizer, running_max, forget_total)


def combine(earlier, latter):
    early_memory, early_norm, early_max, early_total = earlier
    late_memory, late_norm, late_max, late_total = latter
    joint_max = jnp.maximum(early_max + late_total, late_max)
    early_scale = jnp.exp(early_max + late_total - joint_max)
    late_scale = jnp.exp(late_max - joint_max)
    memory = early_scale[:, None, None] * early_memory + late_scale[:, None, None] * late_memory
    normalizer = early_scale[:, None] * early_norm + late_scale[:, None] * late_norm
    return (memory, normalizer, joint_max, early_total + late_total)


def span_sweep(
    query_rows, key_rows, value_rows, input_gate, log_forget, memory, normalizer, stabilizer, span
):
    block_count = query_rows.shape[1] // span

    def to_blocks(array):
        shaped = array.reshape((array.shape[0], block_count, span) + array.shape[2:])
        return jnp.moveaxis(shaped, 1, 0)

    def advance(carried, pieces):
        query_blk, key_blk, value_blk, gate_blk, forget_blk = pieces
        result = block_output(
            query_blk, key_blk, value_blk, gate_blk, forget_blk, carried[0], carried[1], carried[2]
        )
        return (combine(carried, block_summary(key_blk, value_blk, gate_blk, forget_blk)), result)

    initial = (memory, normalizer, stabilizer, jnp.zeros_like(stabilizer))
    ignored, outputs = lax.scan(
        advance,
        initial,
        tuple(
            (
                to_blocks(array)
                for array in (query_rows, key_rows, value_rows, input_gate, log_forget)
            )
        ),
    )
    return jnp.moveaxis(outputs, 0, 1).reshape(query_rows.shape[:2] + (value_rows.shape[2],))


def reverse_time(array):
    return jnp.flip(array, axis=1)


def to_heads(matrix, head_count):
    shaped = matrix.reshape(matrix.shape[0], head_count, matrix.shape[1] // head_count)
    return shaped.transpose(1, 0, 2)


def pool_window(padded, positions, channels, seq_len, group_size):
    row_count = positions.shape[0]
    group_index = channels // group_size
    reach_left = jnp.left_shift(jnp.ones_like(group_index), group_index)
    reach_right = reach_left - 1
    window_sum = jnp.zeros((row_count, channels.shape[0]), jnp.float32)
    for offset in range(-HALO, HALO):
        inside = ((offset >= -reach_left) & (offset <= reach_right)).astype(jnp.float32)
        window_sum = window_sum + inside * padded[HALO + offset : HALO + offset + row_count]
    first_pos = jnp.maximum(positions[:, None] - reach_left[None, :], 0)
    last_pos = jnp.minimum(positions[:, None] + reach_right[None, :], seq_len - 1)
    counted = (last_pos - first_pos + 1).astype(jnp.float32)
    centre = padded[HALO : HALO + row_count]
    return (window_sum / counted - centre).astype(jnp.bfloat16)


def per_device(
    tokens,
    norm_gain,
    query_weight,
    key_weight,
    value_weight,
    outgate_weight,
    gate_weight,
    gate_bias,
    decay_extra,
    init_memory,
    init_normalizer,
    head_gain,
    pool_weight,
    mem_out_weight,
    pool_out_weight,
):
    block_len = tokens.shape[1]
    model_width = tokens.shape[2]
    head_count, head_width = head_gain.shape
    span = math.gcd(block_len, 256)
    flattened = tokens[0].astype(jnp.float32)
    normed = (
        flattened
        * lax.rsqrt(jnp.mean(flattened * flattened, axis=-1, keepdims=True) + norm_eps)
        * norm_gain
    ).astype(jnp.bfloat16)
    zero_start = tuple(
        (
            jnp.zeros((block_len, weight.shape[1]), jnp.float32)
            for weight in (query_weight, key_weight, value_weight, outgate_weight, pool_weight)
        )
    )
    zero_start = zero_start + (
        jnp.zeros((model_width, mem_out_weight.shape[1]), jnp.bfloat16),
        jnp.zeros((model_width, pool_out_weight.shape[1]), jnp.bfloat16),
    )
    line_query, line_key, line_value, line_outgate, line_pool, line_mem_out, line_pool_out = (
        lax.all_gather(query_weight, "fs", axis=0, tiled=True),
        lax.all_gather(key_weight, "fs", axis=0, tiled=True),
        lax.all_gather(value_weight, "fs", axis=0, tiled=True),
        lax.all_gather(outgate_weight, "fs", axis=0, tiled=True),
        lax.all_gather(pool_weight, "fs", axis=0, tiled=True),
        lax.all_gather(mem_out_weight, "fs", axis=0, tiled=True),
        lax.all_gather(pool_out_weight, "fs", axis=0, tiled=True),
    )
    pieces = (
        lax.all_gather(line_query, "sp", axis=0, tiled=True),
        lax.all_gather(line_key, "sp", axis=0, tiled=True),
        lax.all_gather(line_value, "sp", axis=0, tiled=True),
        lax.all_gather(line_outgate, "sp", axis=0, tiled=True),
        lax.all_gather(line_pool, "sp", axis=0, tiled=True),
        lax.all_gather(line_mem_out, "sp", axis=0, tiled=True),
        lax.all_gather(line_pool_out, "sp", axis=0, tiled=True),
    )
    partial_sums = tuple(
        (
            jnp.dot(normed, weight_rows, preferred_element_type=jnp.float32)
            for weight_rows in pieces[:5]
        )
    )
    collected = tuple((weight_rows for weight_rows in pieces[5:]))
    folded = partial_sums + collected
    query_proj, key_proj, value_proj, outgate, pool_input = tuple(
        (running.astype(jnp.bfloat16) for running in folded[:5])
    )
    mem_weight_all = folded[5]
    pool_weight_all = folded[6]
    gate_pre = lax.dot_general(
        normed,
        gate_weight.reshape(4 * head_count, model_width),
        (((1,), (1,)), ((), ())),
        preferred_element_type=jnp.float32,
    ) + gate_bias.reshape(4 * head_count)
    gate_pre = gate_pre.reshape(block_len, 4, head_count).transpose(1, 2, 0)
    query_heads = to_heads(query_proj, head_count)
    key_heads = to_heads(key_proj, head_count)
    value_heads = to_heads(value_proj, head_count)
    forward_forget = jax.nn.log_sigmoid(gate_pre[1]) + decay_extra[0, 0]
    backward_forget = jax.nn.log_sigmoid(gate_pre[3]) + decay_extra[0, 1]
    zero_rows = jnp.zeros((head_count,), jnp.float32)
    identity = (
        jnp.zeros((head_count, head_width, head_width), jnp.float32),
        jnp.zeros((head_count, head_width), jnp.float32),
        jnp.full((head_count,), -1e30, jnp.float32),
        zero_rows,
    )
    front_memory, front_norm, front_max, front_total = block_summary(
        key_heads, value_heads, gate_pre[0], forward_forget
    )
    prefix = carried_in(
        (front_memory, front_norm, front_max, front_total), "sp", combine, identity, False
    )
    incoming = combine((init_memory[0, 0], init_normalizer[0, 0], zero_rows, zero_rows), prefix)
    forward_out = span_sweep(
        query_heads,
        key_heads,
        value_heads,
        gate_pre[0],
        forward_forget,
        incoming[0],
        incoming[1],
        incoming[2],
        span,
    )
    back_query = reverse_time(query_heads)
    back_key = reverse_time(key_heads)
    back_value = reverse_time(value_heads)
    back_gate = reverse_time(gate_pre[2])
    back_forget = reverse_time(backward_forget)
    rear_memory, rear_norm, rear_max, rear_total = block_summary(
        back_key, back_value, back_gate, back_forget
    )
    suffix = carried_in(
        (rear_memory, rear_norm, rear_max, rear_total), "sp", combine, identity, True
    )
    back_incoming = combine(
        (init_memory[0, 1], init_normalizer[0, 1], zero_rows, zero_rows), suffix
    )
    backward_out = reverse_time(
        span_sweep(
            back_query,
            back_key,
            back_value,
            back_gate,
            back_forget,
            back_incoming[0],
            back_incoming[1],
            back_incoming[2],
            span,
        )
    )
    summed_dirs = (forward_out + backward_out).transpose(1, 0, 2)
    normed_heads = (
        summed_dirs
        * lax.rsqrt(jnp.mean(summed_dirs * summed_dirs, axis=-1, keepdims=True) + norm_eps)
        * head_gain
    )
    out_gate = jax.nn.sigmoid(
        outgate.astype(jnp.float32).reshape(block_len, head_count, head_width)
    )
    memory_out = (
        (normed_heads * out_gate).astype(jnp.bfloat16).reshape(block_len, head_count * head_width)
    )
    padded = padded_2(pool_input, (("sp", 0),), HALO).astype(jnp.float32)
    feature_count = pool_input.shape[1]
    positions = lax.axis_index("sp") * block_len + jnp.arange(block_len, dtype=jnp.int32)
    channels = lax.axis_index("tp") * feature_count + jnp.arange(feature_count, dtype=jnp.int32)
    pool_out = pool_window(
        padded, positions, channels, block_len * lax.axis_size("sp"), model_width // 4
    )
    own_rows = block_len // lax.axis_size("tp")
    result = lax.dot_general(
        memory_out, mem_weight_all, (((1,), (1,)), ((), ())), preferred_element_type=jnp.float32
    )
    mixed = lax.psum_scatter(
        (
            result
            + lax.dot_general(
                pool_out,
                pool_weight_all,
                (((1,), (1,)), ((), ())),
                preferred_element_type=jnp.float32,
            )
        ).astype(jnp.bfloat16),
        "tp",
        scatter_dimension=0,
        tiled=True,
    )
    return mixed.reshape(1, own_rows, model_width)


def aligned(start, size):
    return pl.ds(pl.multiple_of(start, size), size)


def gather_kernel(n_sp, n_fs, widths, *refs):
    count = len(widths)
    token_ref, decay_ref = refs[:2]
    weight_refs = refs[2 : 2 + count]
    x_ref, decay_out, in_ref, out_ref = refs[2 + count : 6 + count]
    (
        local_sem,
        token_local,
        weight_send,
        weight_recv,
        decay_send,
        decay_recv,
        token_send,
        token_recv,
        swap_send,
        swap_recv,
        row_send,
        row_recv,
        relay_send,
        relay_recv,
    ) = refs[6 + count :]
    sp, fs, tp = (lax.axis_index(name) for name in ("sp", "fs", "tp"))
    other = 1 - tp
    rows = weight_refs[0].shape[0]
    block = token_ref.shape[0]
    half = block // 2
    ups = [lax.rem(sp + k, n_sp) for k in range(n_sp)]
    downs = [lax.rem(sp + n_sp - k, n_sp) for k in range(n_sp)]
    beside = fs + 1 - 2 * lax.rem(fs, 2)
    across = lax.rem(fs + 2, 4)
    peers = (beside, across)

    barrier = pltpu.get_barrier_semaphore()
    for k in range(1, n_sp):
        pl.semaphore_signal(barrier, inc=1, device_id={"sp": ups[k]}, device_id_type=MESH)
    for peer in peers:
        pl.semaphore_signal(barrier, inc=1, device_id={"fs": peer}, device_id_type=MESH)
    pl.semaphore_signal(barrier, inc=1, device_id={"tp": other}, device_id_type=MESH)
    pl.semaphore_wait(barrier, n_sp + 2)

    in_count = count - 2
    in_width = sum(widths[:in_count])

    def landing(i, source_sp):
        at = aligned((source_sp * n_fs + fs) * rows, rows)
        start = sum(widths[:i])
        if i < in_count:
            return in_ref.at[at, pl.ds(start, widths[i])]
        return out_ref.at[at, pl.ds(start - in_width, widths[i])]

    def piece(i, target_sp):
        return weight_refs[i].at[:, aligned(target_sp * widths[i], widths[i])]

    locals_ = []
    for i in range(count):
        locals_.append(pltpu.make_async_copy(piece(i, sp), landing(i, sp), local_sem.at[i]))
    for copy in locals_:
        copy.start()
    own_tokens = pltpu.make_async_copy(
        token_ref, x_ref.at[aligned(sp * block, block)], token_local.at[0]
    )
    own_tokens.start()
    own_decay = pltpu.make_async_copy(decay_ref.at[sp], decay_out.at[sp], token_local.at[1])
    own_decay.start()

    def weight_copy(i, k, target, source):
        return pltpu.make_async_remote_copy(
            src_ref=piece(i, target),
            dst_ref=landing(i, source),
            send_sem=weight_send.at[k - 1, i],
            recv_sem=weight_recv.at[k - 1, i],
            device_id={"sp": target},
            device_id_type=MESH,
        )

    def decay_copy(k, target, source):
        return pltpu.make_async_remote_copy(
            src_ref=decay_ref.at[target],
            dst_ref=decay_out.at[source],
            send_sem=decay_send.at[k - 1],
            recv_sem=decay_recv.at[k - 1],
            device_id={"sp": target},
            device_id_type=MESH,
        )

    def token_copy(source, step):
        at = aligned(source * block + tp * half, half)
        return pltpu.make_async_remote_copy(
            src_ref=token_ref.at[aligned(tp * half, half)] if source is sp else x_ref.at[at],
            dst_ref=x_ref.at[at],
            send_sem=token_send.at[source * 2 + (step + 1) // 2],
            recv_sem=token_recv.at[source],
            device_id={"sp": sp + step},
            device_id_type=MESH,
        )

    def swap_copy(source, side):
        at = x_ref.at[aligned(source * block + side * half, half)]
        return pltpu.make_async_remote_copy(
            src_ref=at,
            dst_ref=at,
            send_sem=swap_send.at[source],
            recv_sem=swap_recv.at[source],
            device_id={"tp": other},
            device_id_type=MESH,
        )

    def row_copies(k, j, at_fs):
        at = aligned((downs[k] * n_fs + at_fs) * rows, rows)
        return [
            pltpu.make_async_remote_copy(
                src_ref=ref.at[at],
                dst_ref=ref.at[at],
                send_sem=row_send.at[k, j, which],
                recv_sem=row_recv.at[k, j, which],
                device_id={"fs": peers[j]},
                device_id_type=MESH,
            )
            for which, ref in enumerate((in_ref, out_ref))
        ]

    def relay_copies(k, j, at_fs):
        part = rows // 2
        at = aligned((downs[k] * n_fs + at_fs) * rows + j * part, part)
        return [
            pltpu.make_async_remote_copy(
                src_ref=ref.at[at],
                dst_ref=ref.at[at],
                send_sem=relay_send.at[k, j, which],
                recv_sem=relay_recv.at[k, j, which],
                device_id={"fs": peers[j]},
                device_id_type=MESH,
            )
            for which, ref in enumerate((in_ref, out_ref))
        ]

    def neighbour_sends(action):
        for step in (1, -1):
            @pl.when((sp + step >= 0) & (sp + step < n_sp))
            def _(step=step):
                action(token_copy(sp, step))

    def arrivals(action, distances):
        for distance in distances:
            for step in (1, -1):
                source = sp - step * distance
                onward = sp + step

                @pl.when((source >= 0) & (source < n_sp))
                def _(source=source, onward=onward, step=step):
                    action(source, onward, step)

    def relay_tokens(source, onward, step):
        token_copy(source, step).wait_recv()
        swap_copy(source, tp).start()

        @pl.when((onward >= 0) & (onward < n_sp))
        def _():
            token_copy(source, step).start()

    def finish_tokens(source, onward, step):
        swap_copy(source, other).wait_recv()
        swap_copy(source, tp).wait_send()

        @pl.when((onward >= 0) & (onward < n_sp))
        def _():
            token_copy(source, step).wait_send()

    for k in range(1, n_sp):
        for i in range(count):
            weight_copy(i, k, ups[k], sp).start()
    for k in range(1, n_sp):
        decay_copy(k, ups[k], sp).start()
    neighbour_sends(lambda copy: copy.start())
    for copy in locals_:
        copy.wait()
    for k in range(n_sp):
        if k:
            for i in range(count):
                weight_copy(i, k, ups[k], downs[k]).wait_recv()
        for j in range(2):
            for copy in row_copies(k, j, fs):
                copy.start()
    for k in range(n_sp):
        for j in range(2):
            for copy in row_copies(k, j, peers[j]):
                copy.wait_recv()
            for copy in relay_copies(k, 1 - j, peers[j]):
                copy.start()
        if k == n_sp - 2:
            arrivals(relay_tokens, (1,))
    arrivals(relay_tokens, range(2, n_sp))
    own_tokens.wait()
    own_decay.wait()
    for k in range(1, n_sp):
        decay_copy(k, ups[k], downs[k]).wait_recv()
    for k in range(n_sp):
        for j in range(2):
            for copy in relay_copies(k, j, 3 - fs):
                copy.wait_recv()
    arrivals(finish_tokens, range(1, n_sp))
    neighbour_sends(lambda copy: copy.wait_send())
    for k in range(1, n_sp):
        for i in range(count):
            weight_copy(i, k, ups[k], sp).wait_send()
        decay_copy(k, ups[k], sp).wait_send()
    for k in range(n_sp):
        for j in range(2):
            for copy in row_copies(k, j, fs):
                copy.wait_send()
            for copy in relay_copies(k, j, peers[1 - j]):
                copy.wait_send()


def gather_all(tokens, decay, weights):
    n_sp, n_fs = lax.axis_size("sp"), lax.axis_size("fs")
    widths = tuple(weight.shape[1] // n_sp for weight in weights)
    block, model_width = tokens.shape
    count = len(weights)
    vmem = pl.BlockSpec(memory_space=pltpu.VMEM)
    dma = pltpu.SemaphoreType.DMA
    return pl.pallas_call(
        functools.partial(gather_kernel, n_sp, n_fs, widths),
        out_shape=(
            jax.ShapeDtypeStruct((n_sp * block, model_width), tokens.dtype),
            jax.ShapeDtypeStruct(decay.shape, decay.dtype),
            jax.ShapeDtypeStruct((model_width, sum(widths[:-2])), tokens.dtype),
            jax.ShapeDtypeStruct((model_width, sum(widths[-2:])), tokens.dtype),
        ),
        in_specs=[pl.BlockSpec(memory_space=pl.ANY)] * (2 + count),
        out_specs=(vmem,) * 4,
        scratch_shapes=[
            dma((count,)),
            dma((2,)),
            dma((n_sp - 1, count)),
            dma((n_sp - 1, count)),
            dma((n_sp - 1,)),
            dma((n_sp - 1,)),
            dma((2 * n_sp,)),
            dma((n_sp,)),
            dma((n_sp,)),
            dma((n_sp,)),
            dma((n_sp, 2, 2)),
            dma((n_sp, 2, 2)),
            dma((n_sp, 2, 2)),
            dma((n_sp, 2, 2)),
        ],
        compiler_params=pltpu.CompilerParams(
            collective_id=0, has_side_effects=True, vmem_limit_bytes=60 * 2**20
        ),
        name="gather_all",
    )(tokens, decay, *weights)


def memory_kernel(
    q_ref, qk_ref, k_ref, v_ref, gate_ref, cols_ref, rows_ref, mem_ref, norm_ref, gain_ref, o_ref
):
    tb = q_ref.shape[0]
    seq = k_ref.shape[0]
    width = q_ref.shape[1]
    scale = width ** (-0.5)
    q = q_ref[...]
    cols = cols_ref[...]
    front_peak, rear_peak = cols[:, 0:1], cols[:, 1:2]
    front_max, rear_max = cols[:, 2:3], cols[:, 3:4]
    rear_own = cols[:, 4:5]
    score = (
        lax.dot_general(
            q, k_ref[...], (((1,), (1,)), ((), ())), preferred_element_type=jnp.float32
        )
        * scale
    )
    t = pl.program_id(0) * tb + lax.broadcasted_iota(jnp.int32, (tb, seq), 0)
    s = lax.broadcasted_iota(jnp.int32, (tb, seq), 1)
    front = s <= t
    weight = (
        jnp.exp(
            jnp.where(front, rows_ref[0:1, :] - front_peak, rows_ref[1:2, :] - rear_peak)
        )
        * score
    )
    front_weight = jnp.where(front, weight, 0.0)
    rear_weight = jnp.where(front, 0.0, weight)
    wide = q.astype(jnp.float32)
    own_score = jnp.sum(wide * qk_ref[...].astype(jnp.float32), axis=1, keepdims=True) * scale
    own_weight = jnp.exp(rear_own - rear_peak) * own_score
    start = t.shape[0] * pl.program_id(0)
    own_value = v_ref[pl.ds(pl.multiple_of(start, tb), tb), :].astype(jnp.float32)
    carry = lax.dot_general(
        wide,
        mem_ref[...],
        (((1,), (1,)), ((), ())),
        precision=exact_mode,
        preferred_element_type=jnp.float32,
    )

    def one(direction, weights, peak, top, extra_num, extra_den):
        decay = jnp.exp(-peak)
        num = decay * carry[:, direction * width : (direction + 1) * width] + jnp.dot(
            weights.astype(jnp.bfloat16), v_ref[...], preferred_element_type=jnp.float32
        )
        den = decay * jnp.sum(
            wide * norm_ref[direction : direction + 1, :], axis=1, keepdims=True
        ) + jnp.sum(weights, axis=1, keepdims=True)
        return (num + extra_num) / jnp.maximum(jnp.abs(den + extra_den), jnp.exp(-top))

    total = one(0, front_weight, front_peak, front_max, 0.0, 0.0) + one(
        1,
        rear_weight,
        rear_peak,
        rear_max,
        own_weight.astype(jnp.bfloat16).astype(jnp.float32) * own_value,
        own_weight,
    )
    normed = (
        total
        * lax.rsqrt(jnp.mean(total * total, axis=-1, keepdims=True) + norm_eps)
        * gain_ref[...]
    )
    o_ref[...] = (normed * jax.nn.sigmoid(gate_ref[...].astype(jnp.float32))).astype(jnp.bfloat16)


def memory_mix(proj, cols, rows, memory, normalizer, gain, width):
    seq = proj.shape[0]
    tb = math.gcd(seq, 256)

    def part(i, whole):
        if whole:
            return pl.BlockSpec((seq, width), lambda t: (0, i))
        return pl.BlockSpec((tb, width), lambda t: (t, i))

    def fixed(array):
        return pl.BlockSpec(array.shape, lambda t: (0, 0))

    return pl.pallas_call(
        memory_kernel,
        grid=(seq // tb,),
        out_shape=jax.ShapeDtypeStruct((seq, width), jnp.bfloat16),
        in_specs=[
            part(0, False),
            part(1, False),
            part(1, True),
            part(2, True),
            part(3, False),
            pl.BlockSpec((tb, cols.shape[1]), lambda t: (t, 0)),
            fixed(rows),
            fixed(memory),
            fixed(normalizer),
            fixed(gain),
        ],
        out_specs=pl.BlockSpec((tb, width), lambda t: (t, 0)),
        name="memory_mix",
    )(proj, proj, proj, proj, proj, cols, rows, memory, normalizer, gain)


def project_kernel(
    n_sp, mem_ref, pool_ref, weight_ref, o_ref,
    give, take, send, land, total, own, swap_send, swap_recv, z_send, z_recv,
):
    sp, tp = lax.axis_index("sp"), lax.axis_index("tp")
    other = 1 - tp
    half = o_ref.shape[0]
    width = o_ref.shape[1]
    split = mem_ref.shape[1]
    tile = math.gcd(width, 512)

    barrier = pltpu.get_barrier_semaphore()
    for k in range(1, n_sp):
        pl.semaphore_signal(
            barrier, inc=1, device_id={"sp": lax.rem(sp + k, n_sp)}, device_id_type=MESH
        )
    pl.semaphore_signal(barrier, inc=1, device_id={"tp": other}, device_id_type=MESH)
    pl.semaphore_wait(barrier, n_sp)

    def product(target, side, c):
        at = aligned(target * 2 * half + side * half, half)
        columns = pl.ds(c * tile, tile)
        dims = (((1,), (1,)), ((), ()))
        return lax.dot_general(
            mem_ref[at, :],
            weight_ref[columns, :split],
            dims,
            preferred_element_type=jnp.float32,
        ) + lax.dot_general(
            pool_ref[at, :],
            weight_ref[columns, split:],
            dims,
            preferred_element_type=jnp.float32,
        )

    def swap(d):
        return pltpu.make_async_remote_copy(
            src_ref=give.at[d],
            dst_ref=take.at[d],
            send_sem=swap_send.at[d],
            recv_sem=swap_recv.at[d],
            device_id={"tp": other},
            device_id_type=MESH,
        )

    low = 1 - (2 * sp) // n_sp
    place = low * sp + (1 - low) * (n_sp - 1 - sp)

    def pass_on(d, up):
        slot = up * n_sp + d
        return pltpu.make_async_remote_copy(
            src_ref=send.at[d],
            dst_ref=land.at[slot],
            send_sem=z_send.at[d],
            recv_sem=z_recv.at[slot],
            device_id={"sp": sp + 2 * up - 1},
            device_id_type=MESH,
        )

    def actual(d):
        return low * d + (1 - low) * (n_sp - 1 - d)

    order = [(d, actual(d)) for d in range(n_sp - 1, -1, -1)]
    tiles = [slice(c * tile, (c + 1) * tile) for c in range(width // tile)]
    for _, target in order:
        for c, at in enumerate(tiles):
            give[target, :, at] = product(target, other, c).astype(jnp.bfloat16)
        swap(target).start()
    for d, target in order:
        swap(target).wait_recv()
        for c, at in enumerate(tiles):
            total[:, at] = product(target, tp, c) + take[target, :, at].astype(jnp.float32)

        @pl.when(place == d)
        def _():
            own[...] = total[...]

        def forward(up, fed, target=target):
            @pl.when(fed)
            def _():
                pass_on(target, up).wait_recv()
                total[...] += land[up * n_sp + target].astype(jnp.float32)

            send[target] = total[...].astype(jnp.bfloat16)
            pass_on(target, up).start()

        @pl.when(place < d)
        def _():
            forward(low, place > 0)

        @pl.when(place > d)
        def _():
            forward(1 - low, place < n_sp - 1)

    for up in (0, 1):
        @pl.when(sp != (n_sp - 1) * (1 - up))
        def _(up=up):
            pass_on(sp, up).wait_recv()
            own[...] += land[up * n_sp + sp].astype(jnp.float32)

    o_ref[...] = own[...].astype(jnp.bfloat16)
    for d, target in order:
        swap(target).wait_send()

        @pl.when(place != d)
        def _(target=target):
            pass_on(target, 0).wait_send()


def project_out(memory_out, pool_out, weight):
    n_sp = lax.axis_size("sp")
    half = memory_out.shape[0] // (2 * n_sp)
    width = weight.shape[0]
    vmem = pl.BlockSpec(memory_space=pltpu.VMEM)
    dma = pltpu.SemaphoreType.DMA
    buffers = pltpu.VMEM((n_sp, half, width), jnp.bfloat16)
    return pl.pallas_call(
        functools.partial(project_kernel, n_sp),
        out_shape=jax.ShapeDtypeStruct((half, width), jnp.bfloat16),
        in_specs=[vmem] * 3,
        out_specs=vmem,
        scratch_shapes=[
            buffers,
            buffers,
            buffers,
            pltpu.VMEM((2 * n_sp, half, width), jnp.bfloat16),
            pltpu.VMEM((half, width), jnp.float32),
            pltpu.VMEM((half, width), jnp.float32),
            dma((n_sp,)),
            dma((n_sp,)),
            dma((n_sp,)),
            dma((2 * n_sp,)),
        ],
        compiler_params=pltpu.CompilerParams(
            collective_id=1, has_side_effects=True, vmem_limit_bytes=40 * 2**20
        ),
        name="project_out",
    )(memory_out, pool_out, weight)


def by_head(
    tokens,
    norm_gain,
    query_weight,
    key_weight,
    value_weight,
    outgate_weight,
    gate_weight,
    gate_bias,
    decay_extra,
    init_memory,
    init_normalizer,
    head_gain,
    pool_weight,
    mem_out_weight,
    pool_out_weight,
):
    model_width = tokens.shape[2]
    width = head_gain.shape[1]
    n_sp = lax.axis_size("sp")
    sp, tp = lax.axis_index("sp"), lax.axis_index("tp")
    everything, decay, in_weight, out_weight = gather_all(
        tokens[0],
        decay_extra[0].transpose(1, 0, 2),
        (
            query_weight,
            key_weight,
            value_weight,
            outgate_weight,
            pool_weight,
            mem_out_weight,
            pool_out_weight,
        ),
    )
    seq = everything.shape[0]
    decay = decay.transpose(1, 0, 2).reshape(2, seq)
    flattened = everything.astype(jnp.float32)
    normed = (
        flattened
        * lax.rsqrt(jnp.mean(flattened * flattened, axis=-1, keepdims=True) + norm_eps)
        * norm_gain
    ).astype(jnp.bfloat16)
    proj = jnp.dot(normed, in_weight, preferred_element_type=jnp.float32).astype(jnp.bfloat16)
    own_gates = lax.dynamic_index_in_dim(gate_weight, sp, 1, keepdims=False)
    own_bias = lax.dynamic_index_in_dim(gate_bias, sp, 1, keepdims=True)
    gate_pre = (
        lax.dot_general(
            own_gates, normed, (((1,), (1,)), ((), ())), preferred_element_type=jnp.float32
        )
        + own_bias
    )
    front_sum = lax.cumsum(jax.nn.log_sigmoid(gate_pre[1]) + decay[0])
    rear_sum = lax.cumsum(jax.nn.log_sigmoid(gate_pre[3]) + decay[1], reverse=True)
    front_level = gate_pre[0] - front_sum
    rear_level = gate_pre[2] - rear_sum
    front_peak = jnp.maximum(lax.cummax(front_level), 0.0)
    rear_peak = jnp.maximum(lax.cummax(rear_level, reverse=True), 0.0)
    rows = jnp.stack([front_level, rear_level])
    cols = jnp.stack(
        [front_peak, rear_peak, front_sum + front_peak, rear_sum + rear_peak, rear_level]
    ).T
    memory = lax.dynamic_index_in_dim(init_memory[0], sp, 1, keepdims=False)
    normalizer = lax.dynamic_index_in_dim(init_normalizer[0], sp, 1, keepdims=False)
    gain = lax.dynamic_slice_in_dim(head_gain, sp, 1, 0)
    memory_out = memory_mix(
        proj, cols, rows, memory.reshape(2 * width, width), normalizer, gain, width
    )
    pool_input = proj[:, 4 * width :]
    features = pool_input.shape[1]
    padded = jnp.pad(pool_input.astype(jnp.float32), ((HALO, HALO), (0, 0)))
    positions = jnp.arange(seq, dtype=jnp.int32)
    channels = (tp * n_sp + sp) * features + jnp.arange(features, dtype=jnp.int32)
    pool_out = pool_window(padded, positions, channels, seq, model_width // 4)
    mixed = project_out(memory_out, pool_out, out_weight)
    return mixed[None]


def solution(mesh):
    placed = (
        P("fs", "sp", None),
        P(),
        P(("sp", "fs"), "tp"),
        P(("sp", "fs"), "tp"),
        P(("sp", "fs"), "tp"),
        P(("sp", "fs"), "tp"),
        P(None, "tp", None),
        P(None, "tp"),
        P("fs", None, "tp", "sp"),
        P("fs", None, "tp", None, None),
        P("fs", None, "tp", None),
        P("tp", None),
        P(("sp", "fs"), "tp"),
        P(("sp", "fs"), "tp"),
        P(("sp", "fs"), "tp"),
    )

    def body(*args):
        heads, width = args[11].shape
        features = args[12].shape[1]
        fits = (
            lax.axis_size("tp") == 2
            and heads == lax.axis_size("sp")
            and heads > 1
            and lax.axis_size("fs") == 4
            and heads % 2 == 0
            and width == 128
            and features % (128 * heads) == 0
            and args[0].shape[1] % 32 == 0
        )
        return (by_head if fits else per_device)(*args)

    return jax.shard_map(
        body,
        mesh=mesh,
        in_specs=placed,
        out_specs=P("fs", ("sp", "tp"), None),
        check_vma=False,
    )
```

```python
import functools
import math

import jax
import jax.numpy as jnp
from jax import lax
from jax.experimental import pallas as pl
from jax.experimental.pallas import tpu as pltpu
from jax.sharding import PartitionSpec as P

MESH = pl.DeviceIdType.MESH

HALO = 8


norm_eps = 1e-06
exact_mode = lax.Precision.HIGHEST


def carried_in(x, axis, combine, identity, reverse):
    length, position = (lax.axis_size(axis), lax.axis_index(axis))
    everything = jax.tree.map(lambda part: lax.all_gather(part, axis), x)
    start = jax.tree.map(
        lambda part, zero: jnp.broadcast_to(jnp.asarray(zero, part.dtype), part.shape), x, identity
    )

    def lap(k, before):
        at = length - 1 - k if reverse else k
        reached = at > position if reverse else at < position
        new = combine(before, jax.tree.map(lambda part: part[at], everything))
        return jax.tree.map(lambda a, b: jnp.where(reached, a, b), new, before)

    return lax.fori_loop(0, length, lap, start)


def padded_2(block, sides, width):
    for axis, dim in sides:
        count = lax.axis_size(axis)
        forward = [(i, i + 1) for i in range(count - 1)]
        backward = [(target, source) for source, target in forward]
        low = lax.ppermute(
            lax.slice_in_dim(block, block.shape[dim] - width, None, axis=dim), axis, forward
        )
        high = lax.ppermute(lax.slice_in_dim(block, 0, width, axis=dim), axis, backward)
        block = jnp.concatenate([low, block, high], axis=dim)
    return block


def block_output(
    query_rows, key_rows, value_rows, input_gate, log_forget, memory, normalizer, stabilizer
):
    block_len = query_rows.shape[1]
    key_scale = key_rows.shape[-1] ** (-0.5)
    lower_mask = jnp.tril(jnp.ones((block_len, block_len), dtype=bool))
    summed = jnp.cumsum(log_forget, axis=-1)
    log_decay = jnp.where(
        lower_mask, summed[:, :, None] - summed[:, None, :] + input_gate[:, None, :], -jnp.inf
    )
    log_carry = stabilizer[:, None] + summed
    running_max = jnp.maximum(log_carry, jnp.max(log_decay, axis=-1))
    scores = (
        jnp.einsum("btd,bsd->bts", query_rows, key_rows, preferred_element_type=jnp.float32)
        * key_scale
    )
    inner_weight = jnp.exp(log_decay - running_max[:, :, None]) * scores
    weight_rounded = inner_weight.astype(jnp.bfloat16)
    carry_weight = jnp.exp(log_carry - running_max)
    query_wide = query_rows.astype(jnp.float32)
    numerator = carry_weight[:, :, None] * jnp.einsum(
        "bed,btd->bte", memory, query_wide, precision=exact_mode
    )
    numerator = numerator + jnp.einsum(
        "bts,bse->bte", weight_rounded, value_rows, preferred_element_type=jnp.float32
    )
    denominator = carry_weight * jnp.einsum(
        "bd,btd->bt", normalizer, query_wide, precision=exact_mode
    )
    denominator = denominator + jnp.sum(inner_weight, axis=-1)
    return numerator / jnp.maximum(jnp.abs(denominator), jnp.exp(-running_max))[:, :, None]


def block_summary(key_rows, value_rows, input_gate, log_forget):
    key_wide = key_rows.astype(jnp.float32) * key_rows.shape[-1] ** (-0.5)
    summed = jnp.cumsum(log_forget, axis=-1)
    forget_total = summed[:, -1]
    log_weight = forget_total[:, None] - summed + input_gate
    running_max = jnp.max(log_weight, axis=-1)
    weights = jnp.exp(log_weight - running_max[:, None])
    memory = jnp.einsum(
        "bse,bsd->bed",
        weights[:, :, None] * value_rows.astype(jnp.float32),
        key_wide,
        precision=exact_mode,
    )
    normalizer = jnp.einsum("bs,bsd->bd", weights, key_wide, precision=exact_mode)
    return (memory, normalizer, running_max, forget_total)


def combine(earlier, latter):
    early_memory, early_norm, early_max, early_total = earlier
    late_memory, late_norm, late_max, late_total = latter
    joint_max = jnp.maximum(early_max + late_total, late_max)
    early_scale = jnp.exp(early_max + late_total - joint_max)
    late_scale = jnp.exp(late_max - joint_max)
    memory = early_scale[:, None, None] * early_memory + late_scale[:, None, None] * late_memory
    normalizer = early_scale[:, None] * early_norm + late_scale[:, None] * late_norm
    return (memory, normalizer, joint_max, early_total + late_total)


def span_sweep(
    query_rows, key_rows, value_rows, input_gate, log_forget, memory, normalizer, stabilizer, span
):
    block_count = query_rows.shape[1] // span

    def to_blocks(array):
        shaped = array.reshape((array.shape[0], block_count, span) + array.shape[2:])
        return jnp.moveaxis(shaped, 1, 0)

    def advance(carried, pieces):
        query_blk, key_blk, value_blk, gate_blk, forget_blk = pieces
        result = block_output(
            query_blk, key_blk, value_blk, gate_blk, forget_blk, carried[0], carried[1], carried[2]
        )
        return (combine(carried, block_summary(key_blk, value_blk, gate_blk, forget_blk)), result)

    initial = (memory, normalizer, stabilizer, jnp.zeros_like(stabilizer))
    ignored, outputs = lax.scan(
        advance,
        initial,
        tuple(
            (
                to_blocks(array)
                for array in (query_rows, key_rows, value_rows, input_gate, log_forget)
            )
        ),
    )
    return jnp.moveaxis(outputs, 0, 1).reshape(query_rows.shape[:2] + (value_rows.shape[2],))


def reverse_time(array):
    return jnp.flip(array, axis=1)


def to_heads(matrix, head_count):
    shaped = matrix.reshape(matrix.shape[0], head_count, matrix.shape[1] // head_count)
    return shaped.transpose(1, 0, 2)


def pool_window(padded, positions, channels, seq_len, group_size):
    row_count = positions.shape[0]
    group_index = channels // group_size
    reach_left = jnp.left_shift(jnp.ones_like(group_index), group_index)
    reach_right = reach_left - 1
    window_sum = jnp.zeros((row_count, channels.shape[0]), jnp.float32)
    for offset in range(-HALO, HALO):
        inside = ((offset >= -reach_left) & (offset <= reach_right)).astype(jnp.float32)
        window_sum = window_sum + inside * padded[HALO + offset : HALO + offset + row_count]
    first_pos = jnp.maximum(positions[:, None] - reach_left[None, :], 0)
    last_pos = jnp.minimum(positions[:, None] + reach_right[None, :], seq_len - 1)
    counted = (last_pos - first_pos + 1).astype(jnp.float32)
    centre = padded[HALO : HALO + row_count]
    return (window_sum / counted - centre).astype(jnp.bfloat16)


def per_device(
    tokens,
    norm_gain,
    query_weight,
    key_weight,
    value_weight,
    outgate_weight,
    gate_weight,
    gate_bias,
    decay_extra,
    init_memory,
    init_normalizer,
    head_gain,
    pool_weight,
    mem_out_weight,
    pool_out_weight,
):
    block_len = tokens.shape[1]
    model_width = tokens.shape[2]
    head_count, head_width = head_gain.shape
    span = math.gcd(block_len, 256)
    flattened = tokens[0].astype(jnp.float32)
    normed = (
        flattened
        * lax.rsqrt(jnp.mean(flattened * flattened, axis=-1, keepdims=True) + norm_eps)
        * norm_gain
    ).astype(jnp.bfloat16)
    zero_start = tuple(
        (
            jnp.zeros((block_len, weight.shape[1]), jnp.float32)
            for weight in (query_weight, key_weight, value_weight, outgate_weight, pool_weight)
        )
    )
    zero_start = zero_start + (
        jnp.zeros((model_width, mem_out_weight.shape[1]), jnp.bfloat16),
        jnp.zeros((model_width, pool_out_weight.shape[1]), jnp.bfloat16),
    )
    line_query, line_key, line_value, line_outgate, line_pool, line_mem_out, line_pool_out = (
        lax.all_gather(query_weight, "fs", axis=0, tiled=True),
        lax.all_gather(key_weight, "fs", axis=0, tiled=True),
        lax.all_gather(value_weight, "fs", axis=0, tiled=True),
        lax.all_gather(outgate_weight, "fs", axis=0, tiled=True),
        lax.all_gather(pool_weight, "fs", axis=0, tiled=True),
        lax.all_gather(mem_out_weight, "fs", axis=0, tiled=True),
        lax.all_gather(pool_out_weight, "fs", axis=0, tiled=True),
    )
    pieces = (
        lax.all_gather(line_query, "sp", axis=0, tiled=True),
        lax.all_gather(line_key, "sp", axis=0, tiled=True),
        lax.all_gather(line_value, "sp", axis=0, tiled=True),
        lax.all_gather(line_outgate, "sp", axis=0, tiled=True),
        lax.all_gather(line_pool, "sp", axis=0, tiled=True),
        lax.all_gather(line_mem_out, "sp", axis=0, tiled=True),
        lax.all_gather(line_pool_out, "sp", axis=0, tiled=True),
    )
    partial_sums = tuple(
        (
            jnp.dot(normed, weight_rows, preferred_element_type=jnp.float32)
            for weight_rows in pieces[:5]
        )
    )
    collected = tuple((weight_rows for weight_rows in pieces[5:]))
    folded = partial_sums + collected
    query_proj, key_proj, value_proj, outgate, pool_input = tuple(
        (running.astype(jnp.bfloat16) for running in folded[:5])
    )
    mem_weight_all = folded[5]
    pool_weight_all = folded[6]
    gate_pre = lax.dot_general(
        normed,
        gate_weight.reshape(4 * head_count, model_width),
        (((1,), (1,)), ((), ())),
        preferred_element_type=jnp.float32,
    ) + gate_bias.reshape(4 * head_count)
    gate_pre = gate_pre.reshape(block_len, 4, head_count).transpose(1, 2, 0)
    query_heads = to_heads(query_proj, head_count)
    key_heads = to_heads(key_proj, head_count)
    value_heads = to_heads(value_proj, head_count)
    forward_forget = jax.nn.log_sigmoid(gate_pre[1]) + decay_extra[0, 0]
    backward_forget = jax.nn.log_sigmoid(gate_pre[3]) + decay_extra[0, 1]
    zero_rows = jnp.zeros((head_count,), jnp.float32)
    identity = (
        jnp.zeros((head_count, head_width, head_width), jnp.float32),
        jnp.zeros((head_count, head_width), jnp.float32),
        jnp.full((head_count,), -1e30, jnp.float32),
        zero_rows,
    )
    front_memory, front_norm, front_max, front_total = block_summary(
        key_heads, value_heads, gate_pre[0], forward_forget
    )
    prefix = carried_in(
        (front_memory, front_norm, front_max, front_total), "sp", combine, identity, False
    )
    incoming = combine((init_memory[0, 0], init_normalizer[0, 0], zero_rows, zero_rows), prefix)
    forward_out = span_sweep(
        query_heads,
        key_heads,
        value_heads,
        gate_pre[0],
        forward_forget,
        incoming[0],
        incoming[1],
        incoming[2],
        span,
    )
    back_query = reverse_time(query_heads)
    back_key = reverse_time(key_heads)
    back_value = reverse_time(value_heads)
    back_gate = reverse_time(gate_pre[2])
    back_forget = reverse_time(backward_forget)
    rear_memory, rear_norm, rear_max, rear_total = block_summary(
        back_key, back_value, back_gate, back_forget
    )
    suffix = carried_in(
        (rear_memory, rear_norm, rear_max, rear_total), "sp", combine, identity, True
    )
    back_incoming = combine(
        (init_memory[0, 1], init_normalizer[0, 1], zero_rows, zero_rows), suffix
    )
    backward_out = reverse_time(
        span_sweep(
            back_query,
            back_key,
            back_value,
            back_gate,
            back_forget,
            back_incoming[0],
            back_incoming[1],
            back_incoming[2],
            span,
        )
    )
    summed_dirs = (forward_out + backward_out).transpose(1, 0, 2)
    normed_heads = (
        summed_dirs
        * lax.rsqrt(jnp.mean(summed_dirs * summed_dirs, axis=-1, keepdims=True) + norm_eps)
        * head_gain
    )
    out_gate = jax.nn.sigmoid(
        outgate.astype(jnp.float32).reshape(block_len, head_count, head_width)
    )
    memory_out = (
        (normed_heads * out_gate).astype(jnp.bfloat16).reshape(block_len, head_count * head_width)
    )
    padded = padded_2(pool_input, (("sp", 0),), HALO).astype(jnp.float32)
    feature_count = pool_input.shape[1]
    positions = lax.axis_index("sp") * block_len + jnp.arange(block_len, dtype=jnp.int32)
    channels = lax.axis_index("tp") * feature_count + jnp.arange(feature_count, dtype=jnp.int32)
    pool_out = pool_window(
        padded, positions, channels, block_len * lax.axis_size("sp"), model_width // 4
    )
    own_rows = block_len // lax.axis_size("tp")
    result = lax.dot_general(
        memory_out, mem_weight_all, (((1,), (1,)), ((), ())), preferred_element_type=jnp.float32
    )
    mixed = lax.psum_scatter(
        (
            result
            + lax.dot_general(
                pool_out,
                pool_weight_all,
                (((1,), (1,)), ((), ())),
                preferred_element_type=jnp.float32,
            )
        ).astype(jnp.bfloat16),
        "tp",
        scatter_dimension=0,
        tiled=True,
    )
    return mixed.reshape(1, own_rows, model_width)


def aligned(start, size):
    return pl.ds(pl.multiple_of(start, size), size)


def gather_kernel(n_sp, n_fs, widths, *refs):
    count = len(widths)
    token_ref, decay_ref = refs[:2]
    weight_refs = refs[2 : 2 + count]
    x_ref, decay_out, in_ref, out_ref = refs[2 + count : 6 + count]
    (
        local_sem,
        token_local,
        weight_send,
        weight_recv,
        decay_send,
        decay_recv,
        token_send,
        token_recv,
        swap_send,
        swap_recv,
        row_send,
        row_recv,
        relay_send,
        relay_recv,
    ) = refs[6 + count :]
    sp, fs, tp = (lax.axis_index(name) for name in ("sp", "fs", "tp"))
    other = 1 - tp
    rows = weight_refs[0].shape[0]
    block = token_ref.shape[0]
    half = block // 2
    ups = [lax.rem(sp + k, n_sp) for k in range(n_sp)]
    downs = [lax.rem(sp + n_sp - k, n_sp) for k in range(n_sp)]
    beside = fs + 1 - 2 * lax.rem(fs, 2)
    across = lax.rem(fs + 2, 4)
    peers = (beside, across)

    barrier = pltpu.get_barrier_semaphore()
    for k in range(1, n_sp):
        pl.semaphore_signal(barrier, inc=1, device_id={"sp": ups[k]}, device_id_type=MESH)
    for peer in peers:
        pl.semaphore_signal(barrier, inc=1, device_id={"fs": peer}, device_id_type=MESH)
    pl.semaphore_signal(barrier, inc=1, device_id={"tp": other}, device_id_type=MESH)
    pl.semaphore_wait(barrier, n_sp + 2)

    in_count = count - 2
    in_width = sum(widths[:in_count])

    def landing(i, source_sp):
        at = aligned((source_sp * n_fs + fs) * rows, rows)
        start = sum(widths[:i])
        if i < in_count:
            return in_ref.at[at, pl.ds(start, widths[i])]
        return out_ref.at[at, pl.ds(start - in_width, widths[i])]

    def piece(i, target_sp):
        return weight_refs[i].at[:, aligned(target_sp * widths[i], widths[i])]

    locals_ = []
    for i in range(count):
        locals_.append(pltpu.make_async_copy(piece(i, sp), landing(i, sp), local_sem.at[i]))
    for copy in locals_:
        copy.start()
    own_tokens = pltpu.make_async_copy(
        token_ref, x_ref.at[aligned(sp * block, block)], token_local.at[0]
    )
    own_tokens.start()
    own_decay = pltpu.make_async_copy(decay_ref.at[sp], decay_out.at[sp], token_local.at[1])
    own_decay.start()

    def weight_copy(i, k, target, source):
        return pltpu.make_async_remote_copy(
            src_ref=piece(i, target),
            dst_ref=landing(i, source),
            send_sem=weight_send.at[k - 1, i],
            recv_sem=weight_recv.at[k - 1, i],
            device_id={"sp": target},
            device_id_type=MESH,
        )

    def decay_copy(k, target, source):
        return pltpu.make_async_remote_copy(
            src_ref=decay_ref.at[target],
            dst_ref=decay_out.at[source],
            send_sem=decay_send.at[k - 1],
            recv_sem=decay_recv.at[k - 1],
            device_id={"sp": target},
            device_id_type=MESH,
        )

    def token_copy(source, step):
        at = aligned(source * block + tp * half, half)
        return pltpu.make_async_remote_copy(
            src_ref=token_ref.at[aligned(tp * half, half)] if source is sp else x_ref.at[at],
            dst_ref=x_ref.at[at],
            send_sem=token_send.at[source * 2 + (step + 1) // 2],
            recv_sem=token_recv.at[source],
            device_id={"sp": sp + step},
            device_id_type=MESH,
        )

    def swap_copy(source, side):
        at = x_ref.at[aligned(source * block + side * half, half)]
        return pltpu.make_async_remote_copy(
            src_ref=at,
            dst_ref=at,
            send_sem=swap_send.at[source],
            recv_sem=swap_recv.at[source],
            device_id={"tp": other},
            device_id_type=MESH,
        )

    def row_copies(k, j, at_fs):
        at = aligned((downs[k] * n_fs + at_fs) * rows, rows)
        return [
            pltpu.make_async_remote_copy(
                src_ref=ref.at[at],
                dst_ref=ref.at[at],
                send_sem=row_send.at[k, j, which],
                recv_sem=row_recv.at[k, j, which],
                device_id={"fs": peers[j]},
                device_id_type=MESH,
            )
            for which, ref in enumerate((in_ref, out_ref))
        ]

    def relay_copies(k, j, at_fs):
        part = rows // 2
        at = aligned((downs[k] * n_fs + at_fs) * rows + j * part, part)
        return [
            pltpu.make_async_remote_copy(
                src_ref=ref.at[at],
                dst_ref=ref.at[at],
                send_sem=relay_send.at[k, j, which],
                recv_sem=relay_recv.at[k, j, which],
                device_id={"fs": peers[j]},
                device_id_type=MESH,
            )
            for which, ref in enumerate((in_ref, out_ref))
        ]

    def neighbour_sends(action):
        for step in (1, -1):
            @pl.when((sp + step >= 0) & (sp + step < n_sp))
            def _(step=step):
                action(token_copy(sp, step))

    def arrivals(action, distances):
        for distance in distances:
            for step in (1, -1):
                source = sp - step * distance
                onward = sp + step

                @pl.when((source >= 0) & (source < n_sp))
                def _(source=source, onward=onward, step=step):
                    action(source, onward, step)

    def relay_tokens(source, onward, step):
        token_copy(source, step).wait_recv()
        swap_copy(source, tp).start()

        @pl.when((onward >= 0) & (onward < n_sp))
        def _():
            token_copy(source, step).start()

    def finish_tokens(source, onward, step):
        swap_copy(source, other).wait_recv()
        swap_copy(source, tp).wait_send()

        @pl.when((onward >= 0) & (onward < n_sp))
        def _():
            token_copy(source, step).wait_send()

    for k in range(1, n_sp):
        for i in range(count):
            weight_copy(i, k, ups[k], sp).start()
    for k in range(1, n_sp):
        decay_copy(k, ups[k], sp).start()
    neighbour_sends(lambda copy: copy.start())
    for copy in locals_:
        copy.wait()
    for k in range(n_sp):
        if k:
            for i in range(count):
                weight_copy(i, k, ups[k], downs[k]).wait_recv()
        for j in range(2):
            for copy in row_copies(k, j, fs):
                copy.start()
    for k in range(n_sp):
        for j in range(2):
            for copy in row_copies(k, j, peers[j]):
                copy.wait_recv()
            for copy in relay_copies(k, 1 - j, peers[j]):
                copy.start()
        if k == n_sp - 2:
            arrivals(relay_tokens, (1,))
    arrivals(relay_tokens, range(2, n_sp))
    own_tokens.wait()
    own_decay.wait()
    for k in range(1, n_sp):
        decay_copy(k, ups[k], downs[k]).wait_recv()
    for k in range(n_sp):
        for j in range(2):
            for copy in relay_copies(k, j, 3 - fs):
                copy.wait_recv()
    arrivals(finish_tokens, range(1, n_sp))
    neighbour_sends(lambda copy: copy.wait_send())
    for k in range(1, n_sp):
        for i in range(count):
            weight_copy(i, k, ups[k], sp).wait_send()
        decay_copy(k, ups[k], sp).wait_send()
    for k in range(n_sp):
        for j in range(2):
            for copy in row_copies(k, j, fs):
                copy.wait_send()
            for copy in relay_copies(k, j, peers[1 - j]):
                copy.wait_send()


def gather_all(tokens, decay, weights):
    n_sp, n_fs = lax.axis_size("sp"), lax.axis_size("fs")
    widths = tuple(weight.shape[1] // n_sp for weight in weights)
    block, model_width = tokens.shape
    count = len(weights)
    vmem = pl.BlockSpec(memory_space=pltpu.VMEM)
    dma = pltpu.SemaphoreType.DMA
    return pl.pallas_call(
        functools.partial(gather_kernel, n_sp, n_fs, widths),
        out_shape=(
            jax.ShapeDtypeStruct((n_sp * block, model_width), tokens.dtype),
            jax.ShapeDtypeStruct(decay.shape, decay.dtype),
            jax.ShapeDtypeStruct((model_width, sum(widths[:-2])), tokens.dtype),
            jax.ShapeDtypeStruct((model_width, sum(widths[-2:])), tokens.dtype),
        ),
        in_specs=[pl.BlockSpec(memory_space=pl.ANY)] * (2 + count),
        out_specs=(vmem,) * 4,
        scratch_shapes=[
            dma((count,)),
            dma((2,)),
            dma((n_sp - 1, count)),
            dma((n_sp - 1, count)),
            dma((n_sp - 1,)),
            dma((n_sp - 1,)),
            dma((2 * n_sp,)),
            dma((n_sp,)),
            dma((n_sp,)),
            dma((n_sp,)),
            dma((n_sp, 2, 2)),
            dma((n_sp, 2, 2)),
            dma((n_sp, 2, 2)),
            dma((n_sp, 2, 2)),
        ],
        compiler_params=pltpu.CompilerParams(
            collective_id=0, has_side_effects=True, vmem_limit_bytes=60 * 2**20
        ),
        name="gather_all",
    )(tokens, decay, *weights)


def input_kernel(x_ref, gain_ref, weight_ref, gates_ref, bias_ref, proj_ref, pre_ref):
    wide = x_ref[...].astype(jnp.float32)
    normed = (
        wide
        * lax.rsqrt(jnp.mean(wide * wide, axis=-1, keepdims=True) + norm_eps)
        * gain_ref[...]
    ).astype(jnp.bfloat16)
    proj_ref[...] = jnp.dot(
        normed, weight_ref[...], preferred_element_type=jnp.float32
    ).astype(jnp.bfloat16)
    pre_ref[...] = (
        lax.dot_general(
            normed, gates_ref[...], (((1,), (1,)), ((), ())), preferred_element_type=jnp.float32
        )
        + bias_ref[...]
    )


def project_in(x, norm_gain, weight, gates, bias):
    seq, width = x.shape
    tb = math.gcd(seq, 256)

    def fixed(array):
        return pl.BlockSpec(array.shape, lambda t: (0, 0))

    def rows(columns):
        return pl.BlockSpec((tb, columns), lambda t: (t, 0))

    norm_gain = norm_gain[None]
    return pl.pallas_call(
        input_kernel,
        grid=(seq // tb,),
        out_shape=(
            jax.ShapeDtypeStruct((seq, weight.shape[1]), jnp.bfloat16),
            jax.ShapeDtypeStruct((seq, gates.shape[0]), jnp.float32),
        ),
        in_specs=[rows(width), fixed(norm_gain), fixed(weight), fixed(gates), fixed(bias)],
        out_specs=(rows(weight.shape[1]), rows(gates.shape[0])),
        name="project_in",
    )(x, norm_gain, weight, gates, bias)


def scan_lanes(x, combine_, fill, reverse):
    length = x.shape[1]
    lane = lax.broadcasted_iota(jnp.int32, x.shape, 1)
    d = 1
    while d < length:
        if reverse:
            moved = jnp.where(lane < length - d, pltpu.roll(x, length - d, 1), fill)
        else:
            moved = jnp.where(lane >= d, pltpu.roll(x, d, 1), fill)
        x = combine_(x, moved)
        d *= 2
    return x


def prepare_gates(pre_ref, decay_ref, cols_ref, rows_ref, flat_ref):
    gates = pre_ref[...].T[:8]
    forget = jnp.minimum(gates, 0.0) - jnp.log1p(jnp.exp(-jnp.abs(gates))) + decay_ref[...]
    front_sum = scan_lanes(forget, jnp.add, 0.0, False)[1:2]
    rear_sum = scan_lanes(forget, jnp.add, 0.0, True)[3:4]
    front_level = gates - front_sum
    rear_level = gates - rear_sum
    front_peak = scan_lanes(front_level, jnp.maximum, 0.0, False)[0:1]
    rear_peak = scan_lanes(rear_level, jnp.maximum, 0.0, True)[2:3]
    front_peak = jnp.maximum(front_peak, 0.0)
    rear_peak = jnp.maximum(rear_peak, 0.0)
    rows_ref[0:1, :] = front_level[0:1]
    rows_ref[1:2, :] = rear_level[2:3]
    flat_ref[...] = jnp.zeros_like(flat_ref)
    flat_ref[0:1, :] = front_peak
    flat_ref[1:2, :] = rear_peak
    flat_ref[2:3, :] = front_sum + front_peak
    flat_ref[3:4, :] = rear_sum + rear_peak
    flat_ref[4:5, :] = rear_level[2:3]
    cols_ref[...] = flat_ref[...].T


def memory_kernel(
    q_ref, qk_ref, k_ref, v_ref, gate_ref, pre_ref, decay_ref, mem_ref, norm_ref, gain_ref, o_ref,
    cols_ref, rows_ref, flat_ref,
):
    @pl.when(pl.program_id(0) == 0)
    def _():
        prepare_gates(pre_ref, decay_ref, cols_ref, rows_ref, flat_ref)

    tb = q_ref.shape[0]
    seq = k_ref.shape[0]
    width = q_ref.shape[1]
    scale = width ** (-0.5)
    q = q_ref[...]
    cols = cols_ref[pl.ds(pl.multiple_of(pl.program_id(0) * tb, tb), tb), :]
    front_peak, rear_peak = cols[:, 0:1], cols[:, 1:2]
    front_max, rear_max = cols[:, 2:3], cols[:, 3:4]
    rear_own = cols[:, 4:5]
    score = (
        lax.dot_general(
            q, k_ref[...], (((1,), (1,)), ((), ())), preferred_element_type=jnp.float32
        )
        * scale
    )
    t = pl.program_id(0) * tb + lax.broadcasted_iota(jnp.int32, (tb, seq), 0)
    s = lax.broadcasted_iota(jnp.int32, (tb, seq), 1)
    front = s <= t
    weight = (
        jnp.exp(
            jnp.where(front, rows_ref[0:1, :] - front_peak, rows_ref[1:2, :] - rear_peak)
        )
        * score
    )
    front_weight = jnp.where(front, weight, 0.0)
    rear_weight = jnp.where(front, 0.0, weight)
    wide = q.astype(jnp.float32)
    own_score = jnp.sum(wide * qk_ref[...].astype(jnp.float32), axis=1, keepdims=True) * scale
    own_weight = jnp.exp(rear_own - rear_peak) * own_score
    start = t.shape[0] * pl.program_id(0)
    own_value = v_ref[pl.ds(pl.multiple_of(start, tb), tb), :].astype(jnp.float32)
    carry = lax.dot_general(
        wide,
        mem_ref[...],
        (((1,), (1,)), ((), ())),
        precision=exact_mode,
        preferred_element_type=jnp.float32,
    )

    def one(direction, weights, peak, top, extra_num, extra_den):
        decay = jnp.exp(-peak)
        num = decay * carry[:, direction * width : (direction + 1) * width] + jnp.dot(
            weights.astype(jnp.bfloat16), v_ref[...], preferred_element_type=jnp.float32
        )
        den = decay * jnp.sum(
            wide * norm_ref[direction : direction + 1, :], axis=1, keepdims=True
        ) + jnp.sum(weights, axis=1, keepdims=True)
        return (num + extra_num) / jnp.maximum(jnp.abs(den + extra_den), jnp.exp(-top))

    total = one(0, front_weight, front_peak, front_max, 0.0, 0.0) + one(
        1,
        rear_weight,
        rear_peak,
        rear_max,
        own_weight.astype(jnp.bfloat16).astype(jnp.float32) * own_value,
        own_weight,
    )
    normed = (
        total
        * lax.rsqrt(jnp.mean(total * total, axis=-1, keepdims=True) + norm_eps)
        * gain_ref[...]
    )
    o_ref[...] = (normed * jax.nn.sigmoid(gate_ref[...].astype(jnp.float32))).astype(jnp.bfloat16)


def memory_mix(proj, pre, decay, memory, normalizer, gain, width):
    seq = proj.shape[0]
    tb = math.gcd(seq, 256)

    def part(i, whole):
        if whole:
            return pl.BlockSpec((seq, width), lambda t: (0, i))
        return pl.BlockSpec((tb, width), lambda t: (t, i))

    def fixed(array):
        return pl.BlockSpec(array.shape, lambda t: (0, 0))

    return pl.pallas_call(
        memory_kernel,
        grid=(seq // tb,),
        out_shape=jax.ShapeDtypeStruct((seq, width), jnp.bfloat16),
        in_specs=[
            part(0, False),
            part(1, False),
            part(1, True),
            part(2, True),
            part(3, False),
            fixed(pre),
            fixed(decay),
            fixed(memory),
            fixed(normalizer),
            fixed(gain),
        ],
        out_specs=pl.BlockSpec((tb, width), lambda t: (t, 0)),
        scratch_shapes=[
            pltpu.VMEM((seq, 128), jnp.float32),
            pltpu.VMEM((8, seq), jnp.float32),
            pltpu.VMEM((128, seq), jnp.float32),
        ],
        name="memory_mix",
    )(proj, proj, proj, proj, proj, pre, decay, memory, normalizer, gain)


def project_kernel(
    n_sp, mem_ref, pool_ref, weight_ref, o_ref,
    give, take, send, land, total, own, swap_send, swap_recv, z_send, z_recv,
):
    sp, tp = lax.axis_index("sp"), lax.axis_index("tp")
    other = 1 - tp
    half = o_ref.shape[0]
    width = o_ref.shape[1]
    split = mem_ref.shape[1]
    tile = math.gcd(width, 512)

    barrier = pltpu.get_barrier_semaphore()
    for k in range(1, n_sp):
        pl.semaphore_signal(
            barrier, inc=1, device_id={"sp": lax.rem(sp + k, n_sp)}, device_id_type=MESH
        )
    pl.semaphore_signal(barrier, inc=1, device_id={"tp": other}, device_id_type=MESH)
    pl.semaphore_wait(barrier, n_sp)

    def product(target, side, c):
        at = aligned(target * 2 * half + side * half, half)
        columns = pl.ds(c * tile, tile)
        dims = (((1,), (1,)), ((), ()))
        return lax.dot_general(
            mem_ref[at, :],
            weight_ref[columns, :split],
            dims,
            preferred_element_type=jnp.float32,
        ) + lax.dot_general(
            pool_ref[at, :],
            weight_ref[columns, split:],
            dims,
            preferred_element_type=jnp.float32,
        )

    def swap(d):
        return pltpu.make_async_remote_copy(
            src_ref=give.at[d],
            dst_ref=take.at[d],
            send_sem=swap_send.at[d],
            recv_sem=swap_recv.at[d],
            device_id={"tp": other},
            device_id_type=MESH,
        )

    low = 1 - (2 * sp) // n_sp
    place = low * sp + (1 - low) * (n_sp - 1 - sp)

    def pass_on(d, up):
        slot = up * n_sp + d
        return pltpu.make_async_remote_copy(
            src_ref=send.at[d],
            dst_ref=land.at[slot],
            send_sem=z_send.at[d],
            recv_sem=z_recv.at[slot],
            device_id={"sp": sp + 2 * up - 1},
            device_id_type=MESH,
        )

    def actual(d):
        return low * d + (1 - low) * (n_sp - 1 - d)

    order = [(d, actual(d)) for d in range(n_sp - 1, -1, -1)]
    tiles = [slice(c * tile, (c + 1) * tile) for c in range(width // tile)]
    for _, target in order:
        for c, at in enumerate(tiles):
            give[target, :, at] = product(target, other, c).astype(jnp.bfloat16)
        swap(target).start()
    for d, target in order:
        swap(target).wait_recv()
        for c, at in enumerate(tiles):
            total[:, at] = product(target, tp, c) + take[target, :, at].astype(jnp.float32)

        @pl.when(place == d)
        def _():
            own[...] = total[...]

        def forward(up, fed, target=target):
            @pl.when(fed)
            def _():
                pass_on(target, up).wait_recv()
                total[...] += land[up * n_sp + target].astype(jnp.float32)

            send[target] = total[...].astype(jnp.bfloat16)
            pass_on(target, up).start()

        @pl.when(place < d)
        def _():
            forward(low, place > 0)

        @pl.when(place > d)
        def _():
            forward(1 - low, place < n_sp - 1)

    for up in (0, 1):
        @pl.when(sp != (n_sp - 1) * (1 - up))
        def _(up=up):
            pass_on(sp, up).wait_recv()
            own[...] += land[up * n_sp + sp].astype(jnp.float32)

    o_ref[...] = own[...].astype(jnp.bfloat16)
    for d, target in order:
        swap(target).wait_send()

        @pl.when(place != d)
        def _(target=target):
            pass_on(target, 0).wait_send()


def project_out(memory_out, pool_out, weight):
    n_sp = lax.axis_size("sp")
    half = memory_out.shape[0] // (2 * n_sp)
    width = weight.shape[0]
    vmem = pl.BlockSpec(memory_space=pltpu.VMEM)
    dma = pltpu.SemaphoreType.DMA
    buffers = pltpu.VMEM((n_sp, half, width), jnp.bfloat16)
    return pl.pallas_call(
        functools.partial(project_kernel, n_sp),
        out_shape=jax.ShapeDtypeStruct((half, width), jnp.bfloat16),
        in_specs=[vmem] * 3,
        out_specs=vmem,
        scratch_shapes=[
            buffers,
            buffers,
            buffers,
            pltpu.VMEM((2 * n_sp, half, width), jnp.bfloat16),
            pltpu.VMEM((half, width), jnp.float32),
            pltpu.VMEM((half, width), jnp.float32),
            dma((n_sp,)),
            dma((n_sp,)),
            dma((n_sp,)),
            dma((2 * n_sp,)),
        ],
        compiler_params=pltpu.CompilerParams(
            collective_id=1, has_side_effects=True, vmem_limit_bytes=40 * 2**20
        ),
        name="project_out",
    )(memory_out, pool_out, weight)


def by_head(
    tokens,
    norm_gain,
    query_weight,
    key_weight,
    value_weight,
    outgate_weight,
    gate_weight,
    gate_bias,
    decay_extra,
    init_memory,
    init_normalizer,
    head_gain,
    pool_weight,
    mem_out_weight,
    pool_out_weight,
):
    model_width = tokens.shape[2]
    width = head_gain.shape[1]
    n_sp = lax.axis_size("sp")
    sp, tp = lax.axis_index("sp"), lax.axis_index("tp")
    own_gates = lax.dynamic_index_in_dim(gate_weight, sp, 1, keepdims=False)
    own_gates = jnp.pad(own_gates, ((0, 124), (0, 0)))
    own_bias = lax.dynamic_index_in_dim(gate_bias, sp, 1, keepdims=False)
    own_bias = jnp.pad(own_bias, (0, 124))[None]
    everything, decay, in_weight, out_weight = gather_all(
        tokens[0],
        decay_extra[0].transpose(1, 0, 2),
        (
            query_weight,
            key_weight,
            value_weight,
            outgate_weight,
            pool_weight,
            mem_out_weight,
            pool_out_weight,
        ),
    )
    seq = everything.shape[0]
    decay = decay.transpose(1, 0, 2).reshape(2, 1, seq)
    decay = jnp.pad(decay, ((0, 0), (1, 0), (0, 0))).reshape(4, seq)
    decay = jnp.pad(decay, ((0, 4), (0, 0)))
    proj, pre = project_in(everything, norm_gain, in_weight, own_gates, own_bias)
    memory = lax.dynamic_index_in_dim(init_memory[0], sp, 1, keepdims=False)
    normalizer = lax.dynamic_index_in_dim(init_normalizer[0], sp, 1, keepdims=False)
    gain = lax.dynamic_slice_in_dim(head_gain, sp, 1, 0)
    memory_out = memory_mix(
        proj, pre, decay, memory.reshape(2 * width, width), normalizer, gain, width
    )
    pool_input = proj[:, 4 * width :]
    features = pool_input.shape[1]
    padded = jnp.pad(pool_input.astype(jnp.float32), ((HALO, HALO), (0, 0)))
    positions = jnp.arange(seq, dtype=jnp.int32)
    channels = (tp * n_sp + sp) * features + jnp.arange(features, dtype=jnp.int32)
    pool_out = pool_window(padded, positions, channels, seq, model_width // 4)
    mixed = project_out(memory_out, pool_out, out_weight)
    return mixed[None]


def solution(mesh):
    placed = (
        P("fs", "sp", None),
        P(),
        P(("sp", "fs"), "tp"),
        P(("sp", "fs"), "tp"),
        P(("sp", "fs"), "tp"),
        P(("sp", "fs"), "tp"),
        P(None, "tp", None),
        P(None, "tp"),
        P("fs", None, "tp", "sp"),
        P("fs", None, "tp", None, None),
        P("fs", None, "tp", None),
        P("tp", None),
        P(("sp", "fs"), "tp"),
        P(("sp", "fs"), "tp"),
        P(("sp", "fs"), "tp"),
    )

    def body(*args):
        heads, width = args[11].shape
        features = args[12].shape[1]
        fits = (
            lax.axis_size("tp") == 2
            and heads == lax.axis_size("sp")
            and heads > 1
            and lax.axis_size("fs") == 4
            and heads % 2 == 0
            and width == 128
            and features % (128 * heads) == 0
            and args[0].shape[1] % 32 == 0
        )
        return (by_head if fits else per_device)(*args)

    return jax.shard_map(
        body,
        mesh=mesh,
        in_specs=placed,
        out_specs=P("fs", ("sp", "tp"), None),
        check_vma=False,
    )
```
